32 devices in a mesh: dp: 2 (over x), kv: 8 (over z, y), tp: 2 (over core).
Axes of the slice: x: 2, y: 2, z: 4, core: 2. Of those that a mesh axis runs over, the one named last changes fastest.
Arguments:
- tokens: bfloat16 [48, 2048], P('dp', ('kv', 'tp')), may hold values from -21 to 21
- state: float32 [48, 8, 128, 128], P(('dp', 'kv'), 'tp'), may hold values from -3 to 3
- mix_gain: bfloat16 [2048], P(('kv', 'tp')), may hold values from 0.099609375 to 1.8984375
- w_query: bfloat16 [2048, 1024], P('kv', 'tp'), may hold values from -0.125 to 0.125
- w_key: bfloat16 [2048, 1024], P('kv', 'tp'), may hold values from -0.125 to 0.125
- w_value: bfloat16 [2048, 1024], P('kv', 'tp'), may hold values from -0.125 to 0.125
- w_beta: bfloat16 [2048, 8], P('kv', 'tp'), may hold values from -0.125 to 0.125
- w_decay: bfloat16 [2048, 8], P('kv', 'tp'), may hold values from -0.125 to 0.125
- decay_log: float32 [8], P('tp'), may hold values from -1.5 to 1
- head_gain: bfloat16 [128], replicated, may hold values from 0.099609375 to 1.8984375
- w_out: bfloat16 [1024, 2048], P('tp', 'kv'), may hold values from -0.1875 to 0.1875
- ff_gain: bfloat16 [2048], P(('kv', 'tp')), may hold values from 0.099609375 to 1.8984375
- w_up: bfloat16 [2048, 8192], P(None, ('kv', 'tp')), may hold values from -0.125 to 0.125
- w_down: bfloat16 [8192, 2048], P(('kv', 'tp')), may hold values from -0.09375 to 0.09375
Outputs:
- output: bfloat16 [48, 2048], P('dp', ('kv', 'tp'))
- new_state: float32 [48, 8, 128, 128], P(('dp', 'kv'), 'tp')
The draws below stay inside these ranges and needn't reach their ends.
All inputs are finite; a program needn't handle non-finite values.
Results may differ from the reference program's by a relative error of at most 0.013.
Values may be sent and summed in bfloat16 or wider, within the bound.
No kernel may reach another device: no remote copies, remote signals or barrier semaphores. Data moves between devices by JAX's collectives and lax.ppermute only.
A program may use at most 64 MiB of HBM per device.

```python
import jax
import jax.numpy as jnp
from jax import lax

D = 2048
HEADS = 8
HEAD_DIM = 128
FF = 8192
BATCH = 48
KEYS = 1024
N_TP = 2


def draw_tokens(key, part):
    noise_key = jax.random.fold_in(key, 23)
    columns = jnp.arange(D, dtype=jnp.float32) / D
    entries = jnp.clip(jax.random.normal(noise_key, (BATCH, D), jnp.float32), -4.0, 4.0)
    values = entries * (4.0 ** columns)[None, :] * 0.5
    return values.astype(jnp.bfloat16)


def raised(result, own_key, source, target, parts, factor):
    owner, partner = [(jnp.arange(result.shape[axis_at]) // (result.shape[axis_at] // parts)).reshape([-1 if axis == axis_at else 1 for axis in range(result.ndim)]) for axis_at in (source, target)]
    chosen = jax.random.permutation(own_key, parts)[partner]
    strong = (owner == chosen) | (owner == (partner + parts // 2) % parts)
    return jnp.where(strong, factor * result, result)


def block_levels(rng, dims, split, low, largest):
    def one(position, shards_of):
        steps = jax.random.uniform(jax.random.fold_in(jax.random.fold_in(rng, 6), position), (shards_of,), jnp.float32, low / len(split), largest / len(split))
        return jnp.repeat(jnp.exp(steps), dims[position] // shards_of).reshape((-1,) + (1,) * (len(dims) - position - 1))

    loudness = one(*split[0])
    for cut in split[1:]:
        loudness = loudness * one(*cut)
    return loudness


def gaussian(key, shape, spread, bound, pieces=(), kind=jnp.bfloat16):
    factor_of = block_levels(key, shape, pieces, -0.22, 0.18) if pieces else 1.0
    values = jax.random.normal(key, shape, jnp.float32) * spread * factor_of
    return jnp.minimum(jnp.maximum(values, -bound), bound).astype(kind)


def gaussian_with(rng, extent, deviation, limit, split, heavy, kind=jnp.bfloat16):
    result = deviation * jax.random.normal(rng, extent, jnp.float32)
    if split:
        result = result * block_levels(rng, extent, split, -0.22, 0.18)
    return jnp.clip(raised(result, jax.random.fold_in(rng, 3), *heavy), -limit, limit).astype(kind)


def setup_inputs(seed: int = 0) -> dict:
    key_of = jax.random.split(jax.random.key(seed), 15)
    tokens = draw_tokens(jax.random.fold_in(key_of[14], 71), 0)
    state = gaussian(key_of[1], (BATCH, HEADS, HEAD_DIM, HEAD_DIM), 0.5, 3.0, ((0, 16), (1, 2)), jnp.float32)
    mix_gain = jnp.clip(1.0 + 0.18 * jax.random.normal(key_of[2], (D,), jnp.float32), 0.099609375, 1.8984375).astype(jnp.bfloat16)
    w_query = gaussian(key_of[3], (D, KEYS), D ** -0.5, 0.125, ((0, 8), (1, 2)))
    w_key = gaussian(key_of[4], (D, KEYS), D ** -0.5, 0.125, ((0, 8), (1, 2)))
    w_value = gaussian(key_of[5], (D, KEYS), D ** -0.5, 0.125, ((0, 8), (1, 2)))
    w_beta = gaussian(key_of[6], (D, HEADS), D ** -0.5, 0.125, ((0, 8), (1, 2)))
    w_decay = gaussian(key_of[7], (D, HEADS), D ** -0.5, 0.125, ((0, 8), (1, 2)))
    decay_log = jnp.clip(-1.5 + 2.5 * jax.random.uniform(key_of[8], (HEADS,), jnp.float32) ** block_levels(key_of[8], (HEADS,), ((0, 2),), -0.2, 0.2), -1.5, 1.0)
    head_gain = jnp.clip(1.0 + 0.18 * jax.random.normal(key_of[9], (HEAD_DIM,), jnp.float32), 0.099609375, 1.8984375).astype(jnp.bfloat16)
    w_out = gaussian(key_of[10], (KEYS, D), KEYS ** -0.5, 0.1875, ((0, 2), (1, 8)))
    ff_gain = jnp.clip(1.0 + 0.18 * jax.random.normal(key_of[11], (D,), jnp.float32), 0.099609375, 1.8984375).astype(jnp.bfloat16)
    w_up = gaussian(key_of[12], (D, FF), D ** -0.5, 0.125, ((1, 16),))
    w_down = gaussian_with(key_of[13], (FF, D), FF ** -0.5, 0.09375, ((0, 16),), (0, 1, 16, 2.0))
    return dict(tokens=tokens, state=state, mix_gain=mix_gain, w_query=w_query, w_key=w_key, w_value=w_value, w_beta=w_beta, w_decay=w_decay, decay_log=decay_log, head_gain=head_gain, w_out=w_out, ff_gain=ff_gain, w_up=w_up, w_down=w_down)


def reference(tokens, state, mix_gain, w_query, w_key, w_value, w_beta, w_decay, decay_log, head_gain, w_out, ff_gain, w_up, w_down):
    tokens_float = tokens.astype(jnp.float32)
    mean_square = lax.optimization_barrier(jnp.mean(tokens_float * tokens_float, axis=1, keepdims=True))
    scaled = (tokens_float * mix_gain.astype(jnp.float32)).astype(jnp.bfloat16)
    inverse = lax.rsqrt(mean_square + 1e-06)
    query = inverse * jnp.dot(scaled, w_query, preferred_element_type=jnp.float32)
    key_rows = inverse * jnp.dot(scaled, w_key, preferred_element_type=jnp.float32)
    value = inverse * jnp.dot(scaled, w_value, preferred_element_type=jnp.float32)
    beta = jax.nn.sigmoid(inverse * jnp.dot(scaled, w_beta, preferred_element_type=jnp.float32))
    decay = -jnp.exp(decay_log)[None, :] * jax.nn.softplus(inverse * jnp.dot(scaled, w_decay, preferred_element_type=jnp.float32))
    batch_rows = tokens.shape[0]
    query = query.reshape(batch_rows, HEADS, HEAD_DIM)
    key_rows = key_rows.reshape(batch_rows, HEADS, HEAD_DIM)
    value = value.reshape(batch_rows, HEADS, HEAD_DIM)
    qnorm = query * lax.rsqrt(lax.optimization_barrier(jnp.sum(query * query, axis=-1, keepdims=True)) + 1e-06)
    knorm = key_rows * lax.rsqrt(lax.optimization_barrier(jnp.sum(key_rows * key_rows, axis=-1, keepdims=True)) + 1e-06)
    kept = state * jnp.exp(decay)[:, :, None, None]
    predicted = lax.optimization_barrier(jnp.sum(kept * knorm[:, :, :, None], axis=2))
    new_state = kept + (beta[:, :, None] * knorm)[:, :, :, None] * (value - predicted)[:, :, None, :]
    heads = lax.optimization_barrier(jnp.sum(new_state * qnorm[:, :, :, None], axis=2)) / jnp.sqrt(jnp.float32(HEAD_DIM))
    normed = heads * lax.rsqrt(lax.optimization_barrier(jnp.mean(heads * heads, axis=-1, keepdims=True)) + 1e-06) * head_gain.astype(jnp.float32)
    normed = normed.astype(jnp.bfloat16).reshape(batch_rows, KEYS)
    half_width = KEYS // N_TP
    mixed = jnp.zeros((batch_rows, D), jnp.float32)
    for half_index in range(N_TP):
        lower = half_index * half_width
        product = jnp.dot(normed[:, lower:lower + half_width], w_out[lower:lower + half_width], preferred_element_type=jnp.float32)
        mixed = mixed + product.astype(jnp.bfloat16).astype(jnp.float32)
    resid = (tokens_float + mixed).astype(jnp.bfloat16)
    resid_float = resid.astype(jnp.float32)
    mean_square2 = lax.optimization_barrier(jnp.mean(resid_float * resid_float, axis=1, keepdims=True))
    scaled2 = (resid_float * ff_gain.astype(jnp.float32)).astype(jnp.bfloat16)
    up_rows = jnp.dot(scaled2, w_up, preferred_element_type=jnp.float32) * lax.rsqrt(mean_square2 + 1e-06)
    act = jnp.square(jax.nn.relu(up_rows)).astype(jnp.bfloat16)
    output = (resid_float + jnp.dot(act, w_down, preferred_element_type=jnp.float32)).astype(jnp.bfloat16)
    return (output, new_state)
```

```python
import functools

import jax
import jax.numpy as jnp
from jax import lax
from jax.sharding import PartitionSpec as P

BF = jnp.bfloat16
F32 = jnp.float32


def split_pair(value):
    high = value.astype(BF)
    low = (value - lax.reduce_precision(value, 8, 7)).astype(BF)
    return high, low


def local(
    tokens,
    state,
    mix_gain,
    w_query,
    w_key,
    w_value,
    w_beta,
    w_decay,
    decay_log,
    head_gain,
    w_out,
    ff_gain,
    w_up,
    w_down,
    n_kv,
    n_tp,
):
    rows, width = tokens.shape
    seq, heads, size = state.shape[:3]
    n_all = n_kv * n_tp
    model = width * n_all
    keys = heads * size

    packed = jnp.concatenate([tokens, mix_gain[None, :]], axis=0)
    wide = lax.all_gather(packed, "tp", axis=1, tiled=True)
    tp_at = lax.axis_index("tp")
    out_cols = []
    for step in range(n_tp):
        target = (tp_at + step) % n_tp
        block = lax.dynamic_slice_in_dim(w_out, target * width, width, axis=1)
        if step:
            block = lax.ppermute(block, "tp", [(i, (i + step) % n_tp) for i in range(n_tp)])
        out_cols.append(block)

    wide_float = wide[:rows].astype(F32)
    scaled = (wide_float * wide[rows:].astype(F32)).astype(BF)
    dot = functools.partial(jnp.dot, preferred_element_type=F32)
    gates_part = dot(scaled, jnp.concatenate([w_beta, w_decay], axis=1))
    square_part = jnp.sum(wide_float * wide_float, axis=1, keepdims=True)
    small = jnp.concatenate([gates_part, square_part], axis=1)
    high, low = split_pair(small)
    n_small = small.shape[1]
    pad = jnp.zeros((rows, size - 2 * n_small), BF)
    sent = jnp.concatenate(
        [
            dot(scaled, w_query).astype(BF),
            dot(scaled, w_key).astype(BF),
            dot(scaled, w_value).astype(BF),
            high,
            low,
            pad,
        ],
        axis=1,
    ).reshape(n_kv, seq, 3 * keys + size)
    got = lax.all_to_all(sent, "kv", 0, 0, tiled=False)
    total = jnp.sum(got.astype(F32), axis=0)
    small = total[:, 3 * keys : 3 * keys + n_small] + total[:, 3 * keys + n_small : 3 * keys + 2 * n_small]
    inverse = lax.rsqrt(small[:, 2 * heads :] / model + 1e-06)
    query = (inverse * total[:, :keys]).reshape(seq, heads, size)
    key_rows = (inverse * total[:, keys : 2 * keys]).reshape(seq, heads, size)
    value = (inverse * total[:, 2 * keys : 3 * keys]).reshape(seq, heads, size)
    beta = jax.nn.sigmoid(inverse * small[:, :heads])
    decay = -jnp.exp(decay_log)[None, :] * jax.nn.softplus(inverse * small[:, heads : 2 * heads])
    qnorm = query * lax.rsqrt(jnp.sum(query * query, axis=-1, keepdims=True) + 1e-06)
    knorm = key_rows * lax.rsqrt(jnp.sum(key_rows * key_rows, axis=-1, keepdims=True) + 1e-06)
    kept = state * jnp.exp(decay)[:, :, None, None]
    predicted = jnp.sum(kept * knorm[:, :, :, None], axis=2)
    new_state = kept + (beta[:, :, None] * knorm)[:, :, :, None] * (value - predicted)[:, :, None, :]
    read = jnp.sum(new_state * qnorm[:, :, :, None], axis=2) / jnp.sqrt(jnp.float32(size))
    normed = (
        read
        * lax.rsqrt(jnp.mean(read * read, axis=-1, keepdims=True) + 1e-06)
        * head_gain.astype(F32)
    )
    normed = normed.astype(BF).reshape(seq, keys)
    axes = ("kv", "tp")
    spread = lax.all_to_all(jnp.broadcast_to(normed[None], (n_all, seq, keys)), axes, 0, 0, tiled=False)
    spread = spread.reshape(n_kv, n_tp, seq, keys)
    mixed = 0.0
    for step in range(n_tp):
        heads_of = lax.dynamic_index_in_dim(spread, (tp_at - step) % n_tp, 1, keepdims=False)
        part = dot(heads_of.reshape(rows, keys), out_cols[step])
        mixed = mixed + lax.reduce_precision(part, 8, 7)
    resid = (tokens.astype(F32) + mixed).astype(BF)
    resid_float = resid.astype(F32)
    scaled2 = (resid_float * ff_gain.astype(F32)[None, :]).astype(BF)
    high, low = split_pair(jnp.sum(resid_float * resid_float, axis=1))
    tail_rows = -(-2 * rows // width // 8) * 8
    tail = jnp.concatenate([high, low, jnp.zeros((tail_rows * width - 2 * rows,), BF)])
    tail = tail.reshape(tail_rows, width)
    sent2 = jnp.concatenate([scaled2, tail], axis=0)
    got2 = lax.all_to_all(jnp.broadcast_to(sent2[None], (n_all,) + sent2.shape), axes, 0, 0, tiled=False)
    sums = jnp.sum(got2[:, rows:].reshape(n_all, tail_rows * width)[:, : 2 * rows].astype(F32), axis=0)
    inverse2 = lax.rsqrt((sums[:rows] + sums[rows:]) / model + 1e-06)[:, None]
    whole = got2[:, :rows].transpose(1, 0, 2).reshape(rows, model)
    up_rows = dot(whole, w_up) * inverse2
    act = jnp.square(jax.nn.relu(up_rows)).astype(BF)
    down = dot(act, w_down).astype(BF).reshape(rows, n_all, width).transpose(1, 0, 2)
    got3 = lax.all_to_all(down, axes, 0, 0, tiled=False)
    output = (resid_float + jnp.sum(got3.astype(F32), axis=0)).astype(BF)
    return (output, new_state)


def solution(mesh):
    placed = (
        P("dp", ("kv", "tp")),
        P(("dp", "kv"), "tp", None, None),
        P(("kv", "tp")),
        P("kv", "tp"),
        P("kv", "tp"),
        P("kv", "tp"),
        P("kv", "tp"),
        P("kv", "tp"),
        P("tp"),
        P(),
        P("tp", "kv"),
        P(("kv", "tp")),
        P(None, ("kv", "tp")),
        P(("kv", "tp"), None),
    )
    return jax.shard_map(
        functools.partial(local, n_kv=mesh.shape["kv"], n_tp=mesh.shape["tp"]),
        mesh=mesh,
        in_specs=placed,
        out_specs=(P("dp", ("kv", "tp")), P(("dp", "kv"), "tp", None, None)),
        check_vma=False,
    )
```

```python
import functools

import jax
import jax.numpy as jnp
from jax import lax
from jax.experimental import pallas as pl
from jax.experimental.pallas import tpu as pltpu
from jax.sharding import PartitionSpec as P

BF = jnp.bfloat16
F32 = jnp.float32


def split_pair(value):
    high = value.astype(BF)
    low = (value - lax.reduce_precision(value, 8, 7)).astype(BF)
    return high, low


def plain(
    tokens,
    state,
    mix_gain,
    w_query,
    w_key,
    w_value,
    w_beta,
    w_decay,
    decay_log,
    head_gain,
    w_out,
    ff_gain,
    w_up,
    w_down,
    n_kv,
    n_tp,
):
    rows, width = tokens.shape
    seq, heads, size = state.shape[:3]
    n_all = n_kv * n_tp
    model = width * n_all
    keys = heads * size

    packed = jnp.concatenate([tokens, mix_gain[None, :]], axis=0)
    wide = lax.all_gather(packed, "tp", axis=1, tiled=True)
    tp_at = lax.axis_index("tp")
    out_cols = []
    for step in range(n_tp):
        target = (tp_at + step) % n_tp
        block = lax.dynamic_slice_in_dim(w_out, target * width, width, axis=1)
        if step:
            block = lax.ppermute(block, "tp", [(i, (i + step) % n_tp) for i in range(n_tp)])
        out_cols.append(block)

    wide_float = wide[:rows].astype(F32)
    scaled = (wide_float * wide[rows:].astype(F32)).astype(BF)
    dot = functools.partial(jnp.dot, preferred_element_type=F32)
    gates_part = dot(scaled, jnp.concatenate([w_beta, w_decay], axis=1))
    square_part = jnp.sum(wide_float * wide_float, axis=1, keepdims=True)
    small = jnp.concatenate([gates_part, square_part], axis=1)
    high, low = split_pair(small)
    n_small = small.shape[1]
    pad = jnp.zeros((rows, size - 2 * n_small), BF)
    sent = jnp.concatenate(
        [
            dot(scaled, w_query).astype(BF),
            dot(scaled, w_key).astype(BF),
            dot(scaled, w_value).astype(BF),
            high,
            low,
            pad,
        ],
        axis=1,
    ).reshape(n_kv, seq, 3 * keys + size)
    got = lax.all_to_all(sent, "kv", 0, 0, tiled=False)
    total = jnp.sum(got.astype(F32), axis=0)
    small = total[:, 3 * keys : 3 * keys + n_small] + total[:, 3 * keys + n_small : 3 * keys + 2 * n_small]
    inverse = lax.rsqrt(small[:, 2 * heads :] / model + 1e-06)
    query = (inverse * total[:, :keys]).reshape(seq, heads, size)
    key_rows = (inverse * total[:, keys : 2 * keys]).reshape(seq, heads, size)
    value = (inverse * total[:, 2 * keys : 3 * keys]).reshape(seq, heads, size)
    beta = jax.nn.sigmoid(inverse * small[:, :heads])
    decay = -jnp.exp(decay_log)[None, :] * jax.nn.softplus(inverse * small[:, heads : 2 * heads])
    qnorm = query * lax.rsqrt(jnp.sum(query * query, axis=-1, keepdims=True) + 1e-06)
    knorm = key_rows * lax.rsqrt(jnp.sum(key_rows * key_rows, axis=-1, keepdims=True) + 1e-06)
    kept = state * jnp.exp(decay)[:, :, None, None]
    predicted = jnp.sum(kept * knorm[:, :, :, None], axis=2)
    new_state = kept + (beta[:, :, None] * knorm)[:, :, :, None] * (value - predicted)[:, :, None, :]
    read = jnp.sum(new_state * qnorm[:, :, :, None], axis=2) / jnp.sqrt(jnp.float32(size))
    normed = (
        read
        * lax.rsqrt(jnp.mean(read * read, axis=-1, keepdims=True) + 1e-06)
        * head_gain.astype(F32)
    )
    normed = normed.astype(BF).reshape(seq, keys)
    axes = ("kv", "tp")
    spread = lax.all_to_all(jnp.broadcast_to(normed[None], (n_all, seq, keys)), axes, 0, 0, tiled=False)
    spread = spread.reshape(n_kv, n_tp, seq, keys)
    mixed = 0.0
    for step in range(n_tp):
        heads_of = lax.dynamic_index_in_dim(spread, (tp_at - step) % n_tp, 1, keepdims=False)
        part = dot(heads_of.reshape(rows, keys), out_cols[step])
        mixed = mixed + lax.reduce_precision(part, 8, 7)
    resid = (tokens.astype(F32) + mixed).astype(BF)
    resid_float = resid.astype(F32)
    scaled2 = (resid_float * ff_gain.astype(F32)[None, :]).astype(BF)
    high, low = split_pair(jnp.sum(resid_float * resid_float, axis=1))
    tail_rows = -(-2 * rows // width // 8) * 8
    tail = jnp.concatenate([high, low, jnp.zeros((tail_rows * width - 2 * rows,), BF)])
    tail = tail.reshape(tail_rows, width)
    sent2 = jnp.concatenate([scaled2, tail], axis=0)
    got2 = lax.all_to_all(jnp.broadcast_to(sent2[None], (n_all,) + sent2.shape), axes, 0, 0, tiled=False)
    sums = jnp.sum(got2[:, rows:].reshape(n_all, tail_rows * width)[:, : 2 * rows].astype(F32), axis=0)
    inverse2 = lax.rsqrt((sums[:rows] + sums[rows:]) / model + 1e-06)[:, None]
    whole = got2[:, :rows].transpose(1, 0, 2).reshape(rows, model)
    up_rows = dot(whole, w_up) * inverse2
    act = jnp.square(jax.nn.relu(up_rows)).astype(BF)
    down = dot(act, w_down).astype(BF).reshape(rows, n_all, width).transpose(1, 0, 2)
    got3 = lax.all_to_all(down, axes, 0, 0, tiled=False)
    output = (resid_float + jnp.sum(got3.astype(F32), axis=0)).astype(BF)
    return (output, new_state)


LANES = 128
SHIFT = 64


def stage_kernel(*refs, count, cut):
    sources, targets, sems = refs[:count], refs[count:-1], refs[-1]
    width = targets[-1].shape[1]
    tp_at = lax.axis_index("tp")
    copies = [(source, target) for source, target in zip(sources[:cut], targets[:cut])]
    for source, near in ((sources[cut], tp_at), (sources[cut], 1 - tp_at)):
        copies.append((source.at[:, pl.ds(near * width, width)], targets[len(copies)]))
    copies = [pltpu.make_async_copy(a, b, sems.at[n]) for n, (a, b) in enumerate(copies)]
    for copy in copies:
        copy.start()
    for copy in copies:
        copy.wait()


def load_kernel(*refs):
    count = len(refs) // 2
    sems = refs[-1]
    copies = [pltpu.make_async_copy(refs[n], refs[count + n], sems.at[n]) for n in range(count)]
    for copy in copies:
        copy.start()
    for copy in copies:
        copy.wait()


def project_kernel(
    own_ref,
    other_ref,
    own_gain_ref,
    other_gain_ref,
    wq_ref,
    wk_ref,
    wv_ref,
    wb_ref,
    wd_ref,
    out_ref,
    res_ref,
    pack_ref,
    *,
    n_kv,
    seq,
    heads,
):
    rows = own_ref.shape[0]
    first = lax.axis_index("tp") == 0
    own = own_ref[...].astype(F32)
    other = other_ref[...].astype(F32)
    own_scaled = own * own_gain_ref[...].astype(F32)
    other_scaled = other * other_gain_ref[...].astype(F32)
    scaled = jnp.concatenate(
        [
            jnp.where(first, own_scaled, other_scaled),
            jnp.where(first, other_scaled, own_scaled),
        ],
        axis=1,
    ).astype(BF)
    dot = functools.partial(jnp.dot, preferred_element_type=F32)
    for p, weight_ref in enumerate((wq_ref, wk_ref, wv_ref)):
        product = dot(scaled, weight_ref[...])
        for h in range(heads):
            at = (p * heads + h) * rows
            res_ref[at : at + rows, :] = product[:, h * LANES : (h + 1) * LANES]
    at = lax.broadcasted_iota(jnp.int32, (LANES, heads), 0)
    head = lax.broadcasted_iota(jnp.int32, (LANES, heads), 1)
    place_beta = jnp.where(at == head, 1.0, 0.0).astype(BF)
    place_decay = jnp.where(at == head + heads, 1.0, 0.0).astype(BF)
    gate_weights = (dot(place_beta, wb_ref[...]) + dot(place_decay, wd_ref[...])).astype(BF)
    squares = jnp.sum(own * own + other * other, axis=1, keepdims=True)
    lanes = lax.broadcasted_iota(jnp.int32, (rows, LANES), 1)
    gates = lax.dot_general(
        scaled, gate_weights, (((1,), (1,)), ((), ())), preferred_element_type=F32
    )
    small = gates + jnp.where(lanes == 2 * heads, squares, 0.0)
    high = small.astype(BF).astype(F32)
    res_ref[3 * heads * rows :, :] = high + pltpu.roll(small - high, SHIFT, 1)
    per_seq = 3 * heads + 1
    packet = out_ref.shape[0] // n_kv
    for s in range(seq):
        for j in range(per_seq):
            pack_ref[pl.ds(s * per_seq + j, n_kv, packet), :] = res_ref[
                pl.ds(j * rows + s, n_kv, seq), :
            ]
    for j in range(seq * per_seq, packet):
        pack_ref[pl.ds(j, n_kv, packet), :] = jnp.zeros((n_kv, LANES), F32)
    out_ref[...] = pack_ref[...].astype(BF)


def delta_kernel(
    got_ref,
    state_ref,
    decay_log_ref,
    head_gain_ref,
    ff_gain_ref,
    spread_ref,
    new_ref,
    *,
    n_kv,
    seq,
    heads,
    model,
):
    per_seq = 3 * heads + 1
    packet = got_ref.shape[0] // n_kv
    total = got_ref[:packet].astype(F32)
    for d in range(1, n_kv):
        total = total + got_ref[d * packet : (d + 1) * packet].astype(F32)
    lane = lax.broadcasted_iota(jnp.int32, (1, LANES), 1)
    rate = jnp.zeros((1, LANES), F32)
    for h in range(heads):
        rate = jnp.where(lane == heads + h, decay_log_ref[:, h : h + 1], rate)
    rate = jnp.exp(rate)
    betas, keeps, values, rows = [], [], [], []
    for s in range(seq):
        base = s * per_seq
        small = total[base + 3 * heads : base + per_seq]
        small = small + pltpu.roll(small, LANES - SHIFT, 1)
        inverse = lax.rsqrt(small[:, 2 * heads : 2 * heads + 1] / model + 1e-06)
        gates = inverse * small
        betas.append(jax.nn.sigmoid(gates))
        soft = jnp.maximum(gates, 0.0) + jnp.log1p(jnp.exp(-jnp.abs(gates)))
        keeps.append(jnp.exp(-rate * soft))
        query = inverse * total[base : base + heads]
        key = inverse * total[base + heads : base + 2 * heads]
        values.append(inverse * total[base + 2 * heads : base + 3 * heads])
        rows.append(query * lax.rsqrt(jnp.sum(query * query, axis=1, keepdims=True) + 1e-06))
        rows.append(key * lax.rsqrt(jnp.sum(key * key, axis=1, keepdims=True) + 1e-06))
    count = 2 * heads * seq
    padded = -(-count // 8) * 8
    if padded > count:
        rows.append(jnp.zeros((padded - count, LANES), F32))
    columns = jnp.concatenate(rows, axis=0).T
    reads = []
    for s in range(seq):
        for h in range(heads):
            at = 2 * s * heads + h
            qcol = columns[:, at : at + 1]
            kcol = columns[:, at + heads : at + heads + 1]
            kept = state_ref[s, h] * keeps[s][:, heads + h : heads + h + 1]
            predicted = jnp.sum(kept * kcol, axis=0, keepdims=True)
            change = betas[s][:, h : h + 1] * (values[s][h : h + 1] - predicted)
            new = kept + kcol * change
            new_ref[s, h] = new
            reads.append(jnp.sum(new * qcol, axis=0, keepdims=True))
    read = jnp.concatenate(reads, axis=0) / jnp.sqrt(jnp.float32(LANES))
    normed = (
        read
        * lax.rsqrt(jnp.mean(read * read, axis=1, keepdims=True) + 1e-06)
        * head_gain_ref[...].astype(F32)
    )
    lines = spread_ref.shape[1]
    fill = lines - seq * heads
    sent = jnp.concatenate(
        [normed, jnp.broadcast_to(ff_gain_ref[...].astype(F32), (fill, LANES))], axis=0
    ).astype(BF)
    for d in range(spread_ref.shape[0]):
        spread_ref[d] = sent


def mix_kernel(
    got_ref, tokens_ref, own_ref, other_ref, spread_ref, resid_ref, rows_ref, mixed_ref, *, n_kv, n_tp, seq, heads
):
    lines = got_ref.shape[0] // (n_kv * n_tp)
    rows_ref[...] = got_ref[...].astype(F32)
    dot = functools.partial(jnp.dot, preferred_element_type=F32)
    halves = []
    for t in range(n_tp):
        blocks = []
        for h in range(heads):
            parts = [
                rows_ref[pl.ds(t * lines + s * heads + h, n_kv, n_tp * lines), :] for s in range(seq)
            ]
            blocks.append(jnp.concatenate(parts, axis=0))
        halves.append(jnp.concatenate(blocks, axis=1))
    first = lax.axis_index("tp") == 0
    own = jnp.where(first, halves[0], halves[1]).astype(BF)
    other = jnp.where(first, halves[1], halves[0]).astype(BF)
    mixed = dot(own, own_ref[...]).astype(BF).astype(F32) + dot(other, other_ref[...]).astype(BF).astype(F32)
    for s in range(seq):
        mixed_ref[pl.ds(s, n_kv, seq), :] = mixed[s * n_kv : (s + 1) * n_kv]
    resid = (tokens_ref[...].astype(F32) + mixed_ref[...]).astype(BF)
    resid_ref[...] = resid
    for d in range(spread_ref.shape[0]):
        spread_ref[d] = resid


def feed_kernel(
    got_ref, gains_ref, up_ref, down_hbm_ref, out_ref, down_ref, sem, *, gain_line, model
):
    copy = pltpu.make_async_copy(down_hbm_ref, down_ref, sem)
    copy.start()
    n_all, rows, width = got_ref.shape
    lines = gains_ref.shape[0] // n_all
    squares = jnp.zeros((rows, width), F32)
    blocks = []
    for d in range(n_all):
        block = got_ref[d].astype(F32)
        squares = squares + block * block
        gain = gains_ref[d * lines : (d + 1) * lines].astype(F32)[gain_line : gain_line + 1]
        blocks.append((block * gain).astype(BF))
    inverse = lax.rsqrt(jnp.sum(squares, axis=1, keepdims=True) / model + 1e-06)
    scaled = jnp.concatenate(blocks, axis=1)
    up = jnp.dot(scaled, up_ref[...], preferred_element_type=F32) * inverse
    up = jnp.maximum(up, 0.0)
    act = (up * up).astype(BF)
    copy.wait()
    down = jnp.dot(act, down_ref[...], preferred_element_type=F32)
    for d in range(n_all):
        out_ref[d] = down[:, d * width : (d + 1) * width].astype(BF)


def fused(
    tokens,
    state,
    mix_gain,
    w_query,
    w_key,
    w_value,
    w_beta,
    w_decay,
    decay_log,
    head_gain,
    w_out,
    ff_gain,
    w_up,
    w_down,
    n_kv,
    n_tp,
):
    rows, width = tokens.shape
    seq, heads, size = state.shape[:3]
    n_all = n_kv * n_tp
    model = width * n_all
    keys = heads * size
    per_seq = 3 * heads + 1
    packet = -(-seq * per_seq // 8) * 8
    lines = -(-(seq * heads + 1) // 8) * 8
    axes = ("kv", "tp")
    swap = [(i, n_tp - 1 - i) for i in range(n_tp)]
    shape = jax.ShapeDtypeStruct
    vmem = pl.BlockSpec(memory_space=pltpu.VMEM)
    params = pltpu.CompilerParams(vmem_limit_bytes=16 * 1024 * 1024)

    gain_row = mix_gain[None, :]
    other_tokens = lax.ppermute(tokens, "tp", swap)
    other_gain = lax.ppermute(gain_row, "tp", swap)
    hbm = pl.BlockSpec(memory_space=pltpu.HBM)
    in_hbm = functools.partial(pltpu.with_memory_space_constraint, memory_space=pltpu.HBM)
    loaded = (
        w_query,
        w_key,
        w_value,
        w_beta.T,
        w_decay.T,
        tokens,
        gain_row,
        head_gain[None, :],
        ff_gain[None, :],
        decay_log[None, :],
    )
    staged = pl.pallas_call(
        functools.partial(stage_kernel, count=len(loaded) + 1, cut=len(loaded)),
        out_shape=tuple(shape(a.shape, a.dtype) for a in loaded) + (shape((keys, width), BF),) * 2,
        in_specs=[hbm] * (len(loaded) + 1),
        out_specs=(vmem,) * (len(loaded) + 2),
        scratch_shapes=[pltpu.SemaphoreType.DMA((len(loaded) + 2,))],
        name="stage",
        compiler_params=params,
    )(*(in_hbm(a) for a in loaded + (w_out,)))
    w_query, w_key, w_value, w_beta, w_decay, tokens, gain_row, head_gain, ff_gain, decay_log = staged[:-2]
    own_cols, gone_cols = staged[-2:]
    other_cols = lax.ppermute(gone_cols, "tp", swap)

    sent = pl.pallas_call(
        functools.partial(project_kernel, n_kv=n_kv, seq=seq, heads=heads),
        out_shape=shape((n_kv * packet, LANES), BF),
        in_specs=[vmem] * 9,
        out_specs=vmem,
        scratch_shapes=[
            pltpu.VMEM((per_seq * rows, LANES), F32),
            pltpu.VMEM((n_kv * packet, LANES), F32),
        ],
        name="project",
        compiler_params=params,
    )(tokens, other_tokens, gain_row, other_gain, w_query, w_key, w_value, w_beta, w_decay)
    got = lax.all_to_all(sent.reshape(n_kv, packet, LANES), "kv", 0, 0, tiled=False)
    late = lax.optimization_barrier((state, w_up, sent))[:2]
    state, w_up = pl.pallas_call(
        load_kernel,
        out_shape=tuple(shape(a.shape, a.dtype) for a in late),
        in_specs=[hbm] * len(late),
        out_specs=(vmem,) * len(late),
        scratch_shapes=[pltpu.SemaphoreType.DMA((len(late),))],
        name="load",
        compiler_params=params,
    )(*(in_hbm(a) for a in late))
    spread, new_state = pl.pallas_call(
        functools.partial(delta_kernel, n_kv=n_kv, seq=seq, heads=heads, model=model),
        out_shape=(shape((n_all, lines, LANES), BF), shape(state.shape, F32)),
        in_specs=[vmem] * 5,
        out_specs=(vmem, vmem),
        name="delta",
        compiler_params=params,
    )(got.reshape(n_kv * packet, LANES), state, decay_log, head_gain, ff_gain)
    got = lax.all_to_all(spread, axes, 0, 0, tiled=False).reshape(n_all * lines, LANES)
    spread, resid = pl.pallas_call(
        functools.partial(mix_kernel, n_kv=n_kv, n_tp=n_tp, seq=seq, heads=heads),
        out_shape=(shape((n_all, rows, width), BF), shape((rows, width), BF)),
        in_specs=[vmem] * 4,
        out_specs=(vmem, vmem),
        scratch_shapes=[
            pltpu.VMEM((n_all * lines, LANES), F32),
            pltpu.VMEM((rows, width), F32),
        ],
        name="mix",
        compiler_params=params,
    )(got, tokens, own_cols, other_cols)
    got2 = lax.all_to_all(spread, axes, 0, 0, tiled=False)
    down = pl.pallas_call(
        functools.partial(feed_kernel, gain_line=seq * heads, model=model),
        out_shape=shape((n_all, rows, width), BF),
        in_specs=[vmem] * 3 + [hbm],
        out_specs=vmem,
        scratch_shapes=[pltpu.VMEM(w_down.shape, BF), pltpu.SemaphoreType.DMA(())],
        name="feed",
        compiler_params=params,
    )(got2, got, w_up, in_hbm(w_down))
    got3 = lax.all_to_all(down, axes, 0, 0, tiled=False)
    output = (resid.astype(F32) + jnp.sum(got3.astype(F32), axis=0)).astype(BF)
    return (output, new_state)


def local(*arrays, n_kv, n_tp):
    tokens, state = arrays[:2]
    whole_tiles = tokens.shape[1] == LANES and state.shape[2] == LANES and n_kv % 8 == 0 and n_tp == 2
    form = fused if whole_tiles else plain
    return form(*arrays, n_kv=n_kv, n_tp=n_tp)


def solution(mesh):
    placed = (
        P("dp", ("kv", "tp")),
        P(("dp", "kv"), "tp", None, None),
        P(("kv", "tp")),
        P("kv", "tp"),
        P("kv", "tp"),
        P("kv", "tp"),
        P("kv", "tp"),
        P("kv", "tp"),
        P("tp"),
        P(),
        P("tp", "kv"),
        P(("kv", "tp")),
        P(None, ("kv", "tp")),
        P(("kv", "tp"), None),
    )
    return jax.shard_map(
        functools.partial(local, n_kv=mesh.shape["kv"], n_tp=mesh.shape["tp"]),
        mesh=mesh,
        in_specs=placed,
        out_specs=(P("dp", ("kv", "tp")), P(("dp", "kv"), "tp", None, None)),
        check_vma=False,
    )
```

```python
import functools

import jax
import jax.numpy as jnp
from jax import lax
from jax.experimental import pallas as pl
from jax.experimental.pallas import tpu as pltpu
from jax.sharding import PartitionSpec as P

BF = jnp.bfloat16
F32 = jnp.float32


def split_pair(value):
    high = value.astype(BF)
    low = (value - lax.reduce_precision(value, 8, 7)).astype(BF)
    return high, low


def plain(
    tokens,
    state,
    mix_gain,
    w_query,
    w_key,
    w_value,
    w_beta,
    w_decay,
    decay_log,
    head_gain,
    w_out,
    ff_gain,
    w_up,
    w_down,
    n_kv,
    n_tp,
):
    rows, width = tokens.shape
    seq, heads, size = state.shape[:3]
    n_all = n_kv * n_tp
    model = width * n_all
    keys = heads * size

    packed = jnp.concatenate([tokens, mix_gain[None, :]], axis=0)
    wide = lax.all_gather(packed, "tp", axis=1, tiled=True)
    tp_at = lax.axis_index("tp")
    out_cols = []
    for step in range(n_tp):
        target = (tp_at + step) % n_tp
        block = lax.dynamic_slice_in_dim(w_out, target * width, width, axis=1)
        if step:
            block = lax.ppermute(block, "tp", [(i, (i + step) % n_tp) for i in range(n_tp)])
        out_cols.append(block)

    wide_float = wide[:rows].astype(F32)
    scaled = (wide_float * wide[rows:].astype(F32)).astype(BF)
    dot = functools.partial(jnp.dot, preferred_element_type=F32)
    gates_part = dot(scaled, jnp.concatenate([w_beta, w_decay], axis=1))
    square_part = jnp.sum(wide_float * wide_float, axis=1, keepdims=True)
    small = jnp.concatenate([gates_part, square_part], axis=1)
    high, low = split_pair(small)
    n_small = small.shape[1]
    pad = jnp.zeros((rows, size - 2 * n_small), BF)
    sent = jnp.concatenate(
        [
            dot(scaled, w_query).astype(BF),
            dot(scaled, w_key).astype(BF),
            dot(scaled, w_value).astype(BF),
            high,
            low,
            pad,
        ],
        axis=1,
    ).reshape(n_kv, seq, 3 * keys + size)
    got = lax.all_to_all(sent, "kv", 0, 0, tiled=False)
    total = jnp.sum(got.astype(F32), axis=0)
    small = total[:, 3 * keys : 3 * keys + n_small] + total[:, 3 * keys + n_small : 3 * keys + 2 * n_small]
    inverse = lax.rsqrt(small[:, 2 * heads :] / model + 1e-06)
    query = (inverse * total[:, :keys]).reshape(seq, heads, size)
    key_rows = (inverse * total[:, keys : 2 * keys]).reshape(seq, heads, size)
    value = (inverse * total[:, 2 * keys : 3 * keys]).reshape(seq, heads, size)
    beta = jax.nn.sigmoid(inverse * small[:, :heads])
    decay = -jnp.exp(decay_log)[None, :] * jax.nn.softplus(inverse * small[:, heads : 2 * heads])
    qnorm = query * lax.rsqrt(jnp.sum(query * query, axis=-1, keepdims=True) + 1e-06)
    knorm = key_rows * lax.rsqrt(jnp.sum(key_rows * key_rows, axis=-1, keepdims=True) + 1e-06)
    kept = state * jnp.exp(decay)[:, :, None, None]
    predicted = jnp.sum(kept * knorm[:, :, :, None], axis=2)
    new_state = kept + (beta[:, :, None] * knorm)[:, :, :, None] * (value - predicted)[:, :, None, :]
    read = jnp.sum(new_state * qnorm[:, :, :, None], axis=2) / jnp.sqrt(jnp.float32(size))
    normed = (
        read
        * lax.rsqrt(jnp.mean(read * read, axis=-1, keepdims=True) + 1e-06)
        * head_gain.astype(F32)
    )
    normed = normed.astype(BF).reshape(seq, keys)
    axes = ("kv", "tp")
    spread = lax.all_to_all(jnp.broadcast_to(normed[None], (n_all, seq, keys)), axes, 0, 0, tiled=False)
    spread = spread.reshape(n_kv, n_tp, seq, keys)
    mixed = 0.0
    for step in range(n_tp):
        heads_of = lax.dynamic_index_in_dim(spread, (tp_at - step) % n_tp, 1, keepdims=False)
        part = dot(heads_of.reshape(rows, keys), out_cols[step])
        mixed = mixed + lax.reduce_precision(part, 8, 7)
    resid = (tokens.astype(F32) + mixed).astype(BF)
    resid_float = resid.astype(F32)
    scaled2 = (resid_float * ff_gain.astype(F32)[None, :]).astype(BF)
    high, low = split_pair(jnp.sum(resid_float * resid_float, axis=1))
    tail_rows = -(-2 * rows // width // 8) * 8
    tail = jnp.concatenate([high, low, jnp.zeros((tail_rows * width - 2 * rows,), BF)])
    tail = tail.reshape(tail_rows, width)
    sent2 = jnp.concatenate([scaled2, tail], axis=0)
    got2 = lax.all_to_all(jnp.broadcast_to(sent2[None], (n_all,) + sent2.shape), axes, 0, 0, tiled=False)
    sums = jnp.sum(got2[:, rows:].reshape(n_all, tail_rows * width)[:, : 2 * rows].astype(F32), axis=0)
    inverse2 = lax.rsqrt((sums[:rows] + sums[rows:]) / model + 1e-06)[:, None]
    whole = got2[:, :rows].transpose(1, 0, 2).reshape(rows, model)
    up_rows = dot(whole, w_up) * inverse2
    act = jnp.square(jax.nn.relu(up_rows)).astype(BF)
    down = dot(act, w_down).astype(BF).reshape(rows, n_all, width).transpose(1, 0, 2)
    got3 = lax.all_to_all(down, axes, 0, 0, tiled=False)
    output = (resid_float + jnp.sum(got3.astype(F32), axis=0)).astype(BF)
    return (output, new_state)


LANES = 128
SHIFT = 64


def prepare_kernel(
    tokens_ref,
    gain_ref,
    beta_ref,
    decay_ref,
    scaled_ref,
    squares_ref,
    beta_out_ref,
    decay_out_ref,
    tokens_in_ref,
    gain_in_ref,
    sems,
):
    pairs = (
        (tokens_ref, tokens_in_ref),
        (gain_ref, gain_in_ref),
        (beta_ref, beta_out_ref),
        (decay_ref, decay_out_ref),
    )
    copies = [pltpu.make_async_copy(a, b, sems.at[n]) for n, (a, b) in enumerate(pairs)]
    for copy in copies:
        copy.start()
    for copy in copies:
        copy.wait()
    tokens = tokens_in_ref[...].astype(F32)
    scaled_ref[...] = (tokens * gain_in_ref[...].astype(F32)).astype(BF)
    squares_ref[...] = tokens * tokens


def project_kernel(
    own_ref,
    squares_ref,
    other_ref,
    other_gain_ref,
    wq_ref,
    wk_ref,
    wv_ref,
    wb_ref,
    wd_ref,
    out_ref,
    res_ref,
    pack_ref,
    *,
    n_kv,
    seq,
    heads,
):
    rows = own_ref.shape[0]
    first = lax.axis_index("tp") == 0
    own_scaled = own_ref[...].astype(F32)
    other = other_ref[...].astype(F32)
    other_scaled = other * other_gain_ref[...].astype(F32)
    scaled = jnp.concatenate(
        [
            jnp.where(first, own_scaled, other_scaled),
            jnp.where(first, other_scaled, own_scaled),
        ],
        axis=1,
    ).astype(BF)
    dot = functools.partial(jnp.dot, preferred_element_type=F32)
    for p, weight_ref in enumerate((wq_ref, wk_ref, wv_ref)):
        product = dot(scaled, weight_ref[...])
        for h in range(heads):
            at = (p * heads + h) * rows
            res_ref[at : at + rows, :] = product[:, h * LANES : (h + 1) * LANES]
    at = lax.broadcasted_iota(jnp.int32, (LANES, heads), 0)
    head = lax.broadcasted_iota(jnp.int32, (LANES, heads), 1)
    place_beta = jnp.where(at == head, 1.0, 0.0).astype(BF)
    place_decay = jnp.where(at == head + heads, 1.0, 0.0).astype(BF)
    gate_weights = (dot(place_beta, wb_ref[...]) + dot(place_decay, wd_ref[...])).astype(BF)
    squares = jnp.sum(squares_ref[...] + other * other, axis=1, keepdims=True)
    lanes = lax.broadcasted_iota(jnp.int32, (rows, LANES), 1)
    gates = lax.dot_general(
        scaled, gate_weights, (((1,), (1,)), ((), ())), preferred_element_type=F32
    )
    small = gates + jnp.where(lanes == 2 * heads, squares, 0.0)
    high = small.astype(BF).astype(F32)
    res_ref[3 * heads * rows :, :] = high + pltpu.roll(small - high, SHIFT, 1)
    per_seq = 3 * heads + 1
    packet = out_ref.shape[0] // n_kv
    for s in range(seq):
        for j in range(per_seq):
            pack_ref[pl.ds(s * per_seq + j, n_kv, packet), :] = res_ref[
                pl.ds(j * rows + s, n_kv, seq), :
            ]
    for j in range(seq * per_seq, packet):
        pack_ref[pl.ds(j, n_kv, packet), :] = jnp.zeros((n_kv, LANES), F32)
    out_ref[...] = pack_ref[...].astype(BF)


def delta_kernel(
    got_ref,
    state_ref,
    decay_log_ref,
    head_gain_ref,
    ff_gain_ref,
    spread_ref,
    new_ref,
    *,
    n_kv,
    seq,
    heads,
    model,
):
    per_seq = 3 * heads + 1
    packet = got_ref.shape[0] // n_kv
    total = got_ref[:packet].astype(F32)
    for d in range(1, n_kv):
        total = total + got_ref[d * packet : (d + 1) * packet].astype(F32)
    lane = lax.broadcasted_iota(jnp.int32, (1, LANES), 1)
    rate = jnp.zeros((1, LANES), F32)
    for h in range(heads):
        rate = jnp.where(lane == heads + h, decay_log_ref[:, h : h + 1], rate)
    rate = jnp.exp(rate)
    betas, keeps, values, rows = [], [], [], []
    for s in range(seq):
        base = s * per_seq
        small = total[base + 3 * heads : base + per_seq]
        small = small + pltpu.roll(small, LANES - SHIFT, 1)
        inverse = lax.rsqrt(small[:, 2 * heads : 2 * heads + 1] / model + 1e-06)
        gates = inverse * small
        betas.append(jax.nn.sigmoid(gates))
        soft = jnp.maximum(gates, 0.0) + jnp.log1p(jnp.exp(-jnp.abs(gates)))
        keeps.append(jnp.exp(-rate * soft))
        query = inverse * total[base : base + heads]
        key = inverse * total[base + heads : base + 2 * heads]
        values.append(inverse * total[base + 2 * heads : base + 3 * heads])
        rows.append(query * lax.rsqrt(jnp.sum(query * query, axis=1, keepdims=True) + 1e-06))
        rows.append(key * lax.rsqrt(jnp.sum(key * key, axis=1, keepdims=True) + 1e-06))
    count = 2 * heads * seq
    padded = -(-count // 8) * 8
    if padded > count:
        rows.append(jnp.zeros((padded - count, LANES), F32))
    columns = jnp.concatenate(rows, axis=0).T
    reads = []
    for s in range(seq):
        for h in range(heads):
            at = 2 * s * heads + h
            qcol = columns[:, at : at + 1]
            kcol = columns[:, at + heads : at + heads + 1]
            kept = state_ref[s, h] * keeps[s][:, heads + h : heads + h + 1]
            predicted = jnp.sum(kept * kcol, axis=0, keepdims=True)
            change = betas[s][:, h : h + 1] * (values[s][h : h + 1] - predicted)
            new = kept + kcol * change
            new_ref[s, h] = new
            reads.append(jnp.sum(new * qcol, axis=0, keepdims=True))
    read = jnp.concatenate(reads, axis=0) / jnp.sqrt(jnp.float32(LANES))
    normed = (
        read
        * lax.rsqrt(jnp.mean(read * read, axis=1, keepdims=True) + 1e-06)
        * head_gain_ref[...].astype(F32)
    )
    lines = spread_ref.shape[1]
    fill = lines - seq * heads
    sent = jnp.concatenate(
        [normed, jnp.broadcast_to(ff_gain_ref[...].astype(F32), (fill, LANES))], axis=0
    ).astype(BF)
    for d in range(spread_ref.shape[0]):
        spread_ref[d] = sent


def mix_kernel(
    got_ref, tokens_ref, own_ref, other_ref, spread_ref, resid_ref, rows_ref, mixed_ref, *, n_kv, n_tp, seq, heads
):
    lines = got_ref.shape[0] // (n_kv * n_tp)
    rows_ref[...] = got_ref[...].astype(F32)
    dot = functools.partial(jnp.dot, preferred_element_type=F32)
    halves = []
    for t in range(n_tp):
        blocks = []
        for h in range(heads):
            parts = [
                rows_ref[pl.ds(t * n_kv * lines + s * heads + h, n_kv, lines), :] for s in range(seq)
            ]
            blocks.append(jnp.concatenate(parts, axis=0))
        halves.append(jnp.concatenate(blocks, axis=1))
    tp_at = lax.axis_index("tp")
    width = resid_ref.shape[1]
    cols = pl.ds(pl.multiple_of(tp_at * width, width), width)
    first = tp_at == 0
    own = jnp.where(first, halves[0], halves[1]).astype(BF)
    other = jnp.where(first, halves[1], halves[0]).astype(BF)
    mixed = dot(own, own_ref[:, cols]).astype(BF).astype(F32)
    mixed = mixed + dot(other, other_ref[:, cols]).astype(BF).astype(F32)
    for s in range(seq):
        mixed_ref[pl.ds(s, n_kv, seq), :] = mixed[s * n_kv : (s + 1) * n_kv]
    resid = (tokens_ref[...].astype(F32) + mixed_ref[...]).astype(BF)
    resid_ref[...] = resid
    for d in range(spread_ref.shape[0]):
        spread_ref[d] = resid


def feed_kernel(
    got_ref,
    gains_ref,
    up_ref,
    down_ref,
    state_ref,
    out_ref,
    new_ref,
    sem,
    *,
    gain_line,
    model,
    n_tp,
):
    copy = pltpu.make_async_copy(state_ref, new_ref, sem)
    copy.start()
    n_all, rows, width = got_ref.shape
    n_kv = n_all // n_tp
    lines = gains_ref.shape[0] // n_all
    squares = jnp.zeros((rows, width), F32)
    blocks = []
    for at in range(n_all):
        d = (at % n_tp) * n_kv + at // n_tp
        block = got_ref[d].astype(F32)
        squares = squares + block * block
        gain = gains_ref[d * lines : (d + 1) * lines].astype(F32)[gain_line : gain_line + 1]
        blocks.append((block * gain).astype(BF))
    inverse = lax.rsqrt(jnp.sum(squares, axis=1, keepdims=True) / model + 1e-06)
    scaled = jnp.concatenate(blocks, axis=1)
    up = jnp.dot(scaled, up_ref[...], preferred_element_type=F32) * inverse
    up = jnp.maximum(up, 0.0)
    act = (up * up).astype(BF)
    down = jnp.dot(act, down_ref[...], preferred_element_type=F32)
    for at in range(n_all):
        d = (at % n_tp) * n_kv + at // n_tp
        out_ref[d] = down[:, at * width : (at + 1) * width].astype(BF)
    copy.wait()


def fused(
    tokens,
    state,
    mix_gain,
    w_query,
    w_key,
    w_value,
    w_beta,
    w_decay,
    decay_log,
    head_gain,
    w_out,
    ff_gain,
    w_up,
    w_down,
    n_kv,
    n_tp,
):
    rows, width = tokens.shape
    seq, heads, size = state.shape[:3]
    n_all = n_kv * n_tp
    model = width * n_all
    keys = heads * size
    per_seq = 3 * heads + 1
    packet = -(-seq * per_seq // 8) * 8
    lines = -(-(seq * heads + 1) // 8) * 8
    axes = ("tp", "kv")
    swap = [(i, n_tp - 1 - i) for i in range(n_tp)]
    shape = jax.ShapeDtypeStruct
    vmem = pl.BlockSpec(memory_space=pltpu.VMEM)
    cost = pl.CostEstimate(flops=4 * 10**9, bytes_accessed=8 * 10**6, transcendentals=0)
    params = pltpu.CompilerParams(vmem_limit_bytes=16 * 1024 * 1024)

    gain_row = mix_gain[None, :]
    other_tokens = lax.ppermute(tokens, "tp", swap)
    other_gain = lax.ppermute(gain_row, "tp", swap)
    hbm = pl.BlockSpec(memory_space=pltpu.HBM)
    in_hbm = functools.partial(pltpu.with_memory_space_constraint, memory_space=pltpu.HBM)
    other_out = lax.ppermute(w_out, "tp", swap)
    beta_rows, decay_rows = w_beta.T, w_decay.T
    own_scaled, squares, beta_rows, decay_rows = pl.pallas_call(
        prepare_kernel,
        out_shape=(
            shape(tokens.shape, BF),
            shape(tokens.shape, F32),
            shape(beta_rows.shape, BF),
            shape(decay_rows.shape, BF),
        ),
        in_specs=[hbm] * 4,
        out_specs=(vmem,) * 4,
        scratch_shapes=[
            pltpu.VMEM(tokens.shape, BF),
            pltpu.VMEM(gain_row.shape, BF),
            pltpu.SemaphoreType.DMA((4,)),
        ],
        name="prepare",
        cost_estimate=cost,
        compiler_params=params,
    )(in_hbm(tokens), in_hbm(gain_row), in_hbm(beta_rows), in_hbm(decay_rows))

    sent = pl.pallas_call(
        functools.partial(project_kernel, n_kv=n_kv, seq=seq, heads=heads),
        out_shape=shape((n_kv * packet, LANES), BF),
        in_specs=[vmem] * 9,
        out_specs=vmem,
        scratch_shapes=[
            pltpu.VMEM((per_seq * rows, LANES), F32),
            pltpu.VMEM((n_kv * packet, LANES), F32),
        ],
        name="project",
        cost_estimate=cost,
        compiler_params=params,
    )(own_scaled, squares, other_tokens, other_gain, w_query, w_key, w_value, beta_rows, decay_rows)
    sent, other_out = lax.optimization_barrier((sent, other_out))
    got = lax.all_to_all(sent.reshape(n_kv, packet, LANES), "kv", 0, 0, tiled=False)
    spread, new_state = pl.pallas_call(
        functools.partial(delta_kernel, n_kv=n_kv, seq=seq, heads=heads, model=model),
        out_shape=(shape((n_all, lines, LANES), BF), shape(state.shape, F32)),
        in_specs=[vmem] * 5,
        out_specs=(vmem, vmem),
        name="delta",
        cost_estimate=cost,
        compiler_params=params,
    )(got.reshape(n_kv * packet, LANES), state, decay_log[None, :], head_gain[None, :], ff_gain[None, :])
    got = lax.all_to_all(spread, axes, 0, 0, tiled=False).reshape(n_all * lines, LANES)
    spread, resid = pl.pallas_call(
        functools.partial(mix_kernel, n_kv=n_kv, n_tp=n_tp, seq=seq, heads=heads),
        out_shape=(shape((n_all, rows, width), BF), shape((rows, width), BF)),
        in_specs=[vmem] * 4,
        out_specs=(vmem, vmem),
        scratch_shapes=[
            pltpu.VMEM((n_all * lines, LANES), F32),
            pltpu.VMEM((rows, width), F32),
        ],
        name="mix",
        cost_estimate=cost,
        compiler_params=params,
    )(got, tokens, w_out, other_out)
    got2 = lax.all_to_all(spread, axes, 0, 0, tiled=False)
    down, new_state = pl.pallas_call(
        functools.partial(feed_kernel, gain_line=seq * heads, model=model, n_tp=n_tp),
        out_shape=(shape((n_all, rows, width), BF), shape(state.shape, F32)),
        in_specs=[vmem] * 5,
        out_specs=(vmem, hbm),
        scratch_shapes=[pltpu.SemaphoreType.DMA(())],
        name="feed",
        compiler_params=params,
    )(got2, got, w_up, w_down, new_state)
    got3 = lax.all_to_all(down, axes, 0, 0, tiled=False)
    output = (resid.astype(F32) + jnp.sum(got3.astype(F32), axis=0)).astype(BF)
    return (output, new_state)


def local(*arrays, n_kv, n_tp):
    tokens, state = arrays[:2]
    whole_tiles = tokens.shape[1] == LANES and state.shape[2] == LANES and n_kv % 8 == 0 and n_tp == 2
    form = fused if whole_tiles else plain
    return form(*arrays, n_kv=n_kv, n_tp=n_tp)


def solution(mesh):
    placed = (
        P("dp", ("kv", "tp")),
        P(("dp", "kv"), "tp", None, None),
        P(("kv", "tp")),
        P("kv", "tp"),
        P("kv", "tp"),
        P("kv", "tp"),
        P("kv", "tp"),
        P("kv", "tp"),
        P("tp"),
        P(),
        P("tp", "kv"),
        P(("kv", "tp")),
        P(None, ("kv", "tp")),
        P(("kv", "tp"), None),
    )
    return jax.shard_map(
        functools.partial(local, n_kv=mesh.shape["kv"], n_tp=mesh.shape["tp"]),
        mesh=mesh,
        in_specs=placed,
        out_specs=(P("dp", ("kv", "tp")), P(("dp", "kv"), "tp", None, None)),
        check_vma=False,
    )
```

```python
import functools

import jax
import jax.numpy as jnp
from jax import lax
from jax.experimental import pallas as pl
from jax.experimental.pallas import tpu as pltpu
from jax.sharding import PartitionSpec as P

BF = jnp.bfloat16
F32 = jnp.float32


def split_pair(value):
    high = value.astype(BF)
    low = (value - lax.reduce_precision(value, 8, 7)).astype(BF)
    return high, low


def plain(
    tokens,
    state,
    mix_gain,
    w_query,
    w_key,
    w_value,
    w_beta,
    w_decay,
    decay_log,
    head_gain,
    w_out,
    ff_gain,
    w_up,
    w_down,
    n_kv,
    n_tp,
):
    rows, width = tokens.shape
    seq, heads, size = state.shape[:3]
    n_all = n_kv * n_tp
    model = width * n_all
    keys = heads * size

    packed = jnp.concatenate([tokens, mix_gain[None, :]], axis=0)
    wide = lax.all_gather(packed, "tp", axis=1, tiled=True)
    tp_at = lax.axis_index("tp")
    out_cols = []
    for step in range(n_tp):
        target = (tp_at + step) % n_tp
        block = lax.dynamic_slice_in_dim(w_out, target * width, width, axis=1)
        if step:
            block = lax.ppermute(block, "tp", [(i, (i + step) % n_tp) for i in range(n_tp)])
        out_cols.append(block)

    wide_float = wide[:rows].astype(F32)
    scaled = (wide_float * wide[rows:].astype(F32)).astype(BF)
    dot = functools.partial(jnp.dot, preferred_element_type=F32)
    gates_part = dot(scaled, jnp.concatenate([w_beta, w_decay], axis=1))
    square_part = jnp.sum(wide_float * wide_float, axis=1, keepdims=True)
    small = jnp.concatenate([gates_part, square_part], axis=1)
    high, low = split_pair(small)
    n_small = small.shape[1]
    pad = jnp.zeros((rows, size - 2 * n_small), BF)
    sent = jnp.concatenate(
        [
            dot(scaled, w_query).astype(BF),
            dot(scaled, w_key).astype(BF),
            dot(scaled, w_value).astype(BF),
            high,
            low,
            pad,
        ],
        axis=1,
    ).reshape(n_kv, seq, 3 * keys + size)
    got = lax.all_to_all(sent, "kv", 0, 0, tiled=False)
    total = jnp.sum(got.astype(F32), axis=0)
    small = total[:, 3 * keys : 3 * keys + n_small] + total[:, 3 * keys + n_small : 3 * keys + 2 * n_small]
    inverse = lax.rsqrt(small[:, 2 * heads :] / model + 1e-06)
    query = (inverse * total[:, :keys]).reshape(seq, heads, size)
    key_rows = (inverse * total[:, keys : 2 * keys]).reshape(seq, heads, size)
    value = (inverse * total[:, 2 * keys : 3 * keys]).reshape(seq, heads, size)
    beta = jax.nn.sigmoid(inverse * small[:, :heads])
    decay = -jnp.exp(decay_log)[None, :] * jax.nn.softplus(inverse * small[:, heads : 2 * heads])
    qnorm = query * lax.rsqrt(jnp.sum(query * query, axis=-1, keepdims=True) + 1e-06)
    knorm = key_rows * lax.rsqrt(jnp.sum(key_rows * key_rows, axis=-1, keepdims=True) + 1e-06)
    kept = state * jnp.exp(decay)[:, :, None, None]
    predicted = jnp.sum(kept * knorm[:, :, :, None], axis=2)
    new_state = kept + (beta[:, :, None] * knorm)[:, :, :, None] * (value - predicted)[:, :, None, :]
    read = jnp.sum(new_state * qnorm[:, :, :, None], axis=2) / jnp.sqrt(jnp.float32(size))
    normed = (
        read
        * lax.rsqrt(jnp.mean(read * read, axis=-1, keepdims=True) + 1e-06)
        * head_gain.astype(F32)
    )
    normed = normed.astype(BF).reshape(seq, keys)
    axes = ("kv", "tp")
    spread = lax.all_to_all(jnp.broadcast_to(normed[None], (n_all, seq, keys)), axes, 0, 0, tiled=False)
    spread = spread.reshape(n_kv, n_tp, seq, keys)
    mixed = 0.0
    for step in range(n_tp):
        heads_of = lax.dynamic_index_in_dim(spread, (tp_at - step) % n_tp, 1, keepdims=False)
        part = dot(heads_of.reshape(rows, keys), out_cols[step])
        mixed = mixed + lax.reduce_precision(part, 8, 7)
    resid = (tokens.astype(F32) + mixed).astype(BF)
    resid_float = resid.astype(F32)
    scaled2 = (resid_float * ff_gain.astype(F32)[None, :]).astype(BF)
    high, low = split_pair(jnp.sum(resid_float * resid_float, axis=1))
    tail_rows = -(-2 * rows // width // 8) * 8
    tail = jnp.concatenate([high, low, jnp.zeros((tail_rows * width - 2 * rows,), BF)])
    tail = tail.reshape(tail_rows, width)
    sent2 = jnp.concatenate([scaled2, tail], axis=0)
    got2 = lax.all_to_all(jnp.broadcast_to(sent2[None], (n_all,) + sent2.shape), axes, 0, 0, tiled=False)
    sums = jnp.sum(got2[:, rows:].reshape(n_all, tail_rows * width)[:, : 2 * rows].astype(F32), axis=0)
    inverse2 = lax.rsqrt((sums[:rows] + sums[rows:]) / model + 1e-06)[:, None]
    whole = got2[:, :rows].transpose(1, 0, 2).reshape(rows, model)
    up_rows = dot(whole, w_up) * inverse2
    act = jnp.square(jax.nn.relu(up_rows)).astype(BF)
    down = dot(act, w_down).astype(BF).reshape(rows, n_all, width).transpose(1, 0, 2)
    got3 = lax.all_to_all(down, axes, 0, 0, tiled=False)
    output = (resid_float + jnp.sum(got3.astype(F32), axis=0)).astype(BF)
    return (output, new_state)


LANES = 128
SHIFT = 64


def place_kernel(out_ref):
    lane = lax.broadcasted_iota(jnp.int32, out_ref.shape, 0)
    head = lax.broadcasted_iota(jnp.int32, out_ref.shape, 1)
    out_ref[...] = jnp.where(lane == head, 1.0, 0.0).astype(BF)


def packet_line(s, j, seq, heads):
    if j < 2 * heads:
        return 2 * heads * s + j
    if j < 3 * heads:
        return 2 * heads * seq + heads * s + j - 2 * heads
    return 3 * heads * seq + s


def project_kernel(
    place_ref,
    own_ref,
    own_gain_ref,
    other_ref,
    other_gain_ref,
    wq_ref,
    wk_ref,
    wv_ref,
    wb_ref,
    wd_ref,
    out_ref,
    res_ref,
    pack_ref,
    *,
    n_kv,
    seq,
    heads,
):
    rows = own_ref.shape[0]
    first = lax.axis_index("tp") == 0
    own = own_ref[...].astype(F32)
    own_scaled = own * own_gain_ref[...].astype(F32)
    other = other_ref[...].astype(F32)
    other_scaled = other * other_gain_ref[...].astype(F32)
    scaled = jnp.concatenate(
        [
            jnp.where(first, own_scaled, other_scaled),
            jnp.where(first, other_scaled, own_scaled),
        ],
        axis=1,
    ).astype(BF)
    dot = functools.partial(jnp.dot, preferred_element_type=F32)
    for p, weight_ref in enumerate((wq_ref, wk_ref, wv_ref)):
        product = dot(scaled, weight_ref[...])
        for h in range(heads):
            at = (p * heads + h) * rows
            res_ref[at : at + rows, :] = product[:, h * LANES : (h + 1) * LANES]
    gate_weights = dot(place_ref[:, :heads], wb_ref[...])
    gate_weights = (gate_weights + dot(place_ref[:, heads:], wd_ref[...])).astype(BF)
    squares = jnp.sum(own * own + other * other, axis=1, keepdims=True)
    lanes = lax.broadcasted_iota(jnp.int32, (rows, LANES), 1)
    gates = lax.dot_general(
        scaled, gate_weights, (((1,), (1,)), ((), ())), preferred_element_type=F32
    )
    small = gates + jnp.where(lanes == 2 * heads, squares, 0.0)
    high = small.astype(BF).astype(F32)
    res_ref[3 * heads * rows :, :] = high + pltpu.roll(small - high, SHIFT, 1)
    per_seq = 3 * heads + 1
    packet = out_ref.shape[0] // n_kv
    for s in range(seq):
        for j in range(per_seq):
            line = packet_line(s, j, seq, heads)
            pack_ref[pl.ds(line, n_kv, packet), :] = res_ref[pl.ds(j * rows + s, n_kv, seq), :]
    for j in range(seq * per_seq, packet):
        pack_ref[pl.ds(j, n_kv, packet), :] = jnp.zeros((n_kv, LANES), F32)
    out_ref[...] = pack_ref[...].astype(BF)


def delta_kernel(
    got_ref,
    state_ref,
    decay_log_ref,
    head_gain_ref,
    ff_gain_ref,
    spread_ref,
    new_ref,
    *,
    n_kv,
    seq,
    heads,
    model,
):
    packet = got_ref.shape[0] // n_kv
    total = got_ref[:packet].astype(F32)
    for d in range(1, n_kv):
        total = total + got_ref[d * packet : (d + 1) * packet].astype(F32)
    pair = 2 * heads
    stack = total[: pair * seq]
    columns = stack.T
    lengths = jnp.sum(stack * stack, axis=1, keepdims=True)
    first = 3 * heads * seq
    start = first - first % 8
    small = total[start:]
    small = small + pltpu.roll(small, LANES - SHIFT, 1)
    inverses = lax.rsqrt(small[:, pair : pair + 1] / model + 1e-06)
    lane = lax.broadcasted_iota(jnp.int32, (1, LANES), 1)
    rate = jnp.zeros((1, LANES), F32)
    for h in range(heads):
        rate = jnp.where(lane == heads + h, decay_log_ref[:, h : h + 1], rate)
    gates = inverses * small
    betas = jax.nn.sigmoid(gates)
    soft = jnp.maximum(gates, 0.0) + jnp.log1p(jnp.exp(-jnp.abs(gates)))
    keeps = jnp.exp(-jnp.exp(rate) * soft)
    row = lax.broadcasted_iota(jnp.int32, (pair, LANES), 0)
    at_lane = lax.broadcasted_iota(jnp.int32, (pair, LANES), 1)
    head = jnp.where(row < heads, row, row - heads)
    reads = []
    for s in range(seq):
        line = first - start + s
        inverse = inverses[line : line + 1]
        beta = jnp.where(at_lane == head, betas[line : line + 1], 0.0)
        beta = jnp.sum(beta, axis=1, keepdims=True)
        keep = jnp.where(at_lane == head + heads, keeps[line : line + 1], 0.0)
        keep = jnp.sum(keep, axis=1, keepdims=True)
        vectors = stack[pair * s : pair * (s + 1)]
        length = lengths[pair * s : pair * (s + 1)]
        scale = inverse * lax.rsqrt(inverse * inverse * length + 1e-06)
        high = vectors.astype(BF)
        low = (vectors - high.astype(F32)).astype(BF)
        parts = jnp.concatenate([high, low], axis=0)
        found = jnp.zeros((pair, LANES), F32)
        for h in range(heads):
            block = state_ref[s, h]
            near = block.astype(BF)
            rest = (block - near.astype(F32)).astype(BF)
            both = jnp.dot(parts, near, preferred_element_type=F32)
            both = both + jnp.dot(parts, rest, preferred_element_type=F32)
            found = jnp.where(head == h, both[:pair] + both[pair:], found)
        found = found * (keep * scale)
        value = inverse * total[pair * seq + heads * s : pair * seq + heads * (s + 1)]
        change = (beta[:heads] * scale[heads:]) * (value - found[heads:])
        cross = jnp.sum(vectors[:heads] * vectors[heads:], axis=1, keepdims=True)
        reads.append(found[:heads] + (scale[:heads] * cross) * change)
        for h in range(heads):
            kcol = columns[:, pair * s + heads + h : pair * s + heads + h + 1]
            new_ref[s, h] = keep[h : h + 1] * state_ref[s, h] + kcol * change[h : h + 1]
    read = jnp.concatenate(reads, axis=0) / jnp.sqrt(jnp.float32(LANES))
    normed = (
        read
        * lax.rsqrt(jnp.mean(read * read, axis=1, keepdims=True) + 1e-06)
        * head_gain_ref[...].astype(F32)
    )
    lines = spread_ref.shape[1]
    fill = lines - seq * heads
    sent = jnp.concatenate(
        [normed, jnp.broadcast_to(ff_gain_ref[...].astype(F32), (fill, LANES))], axis=0
    ).astype(BF)
    for d in range(spread_ref.shape[0]):
        spread_ref[d] = sent


def mix_kernel(
    got_ref, tokens_ref, own_ref, other_ref, spread_ref, resid_ref, rows_ref, mixed_ref, *, n_kv, n_tp, seq, heads
):
    lines = got_ref.shape[0] // (n_kv * n_tp)
    rows_ref[...] = got_ref[...].astype(F32)
    dot = functools.partial(jnp.dot, preferred_element_type=F32)
    halves = []
    for t in range(n_tp):
        blocks = []
        for h in range(heads):
            parts = [
                rows_ref[pl.ds(t * n_kv * lines + s * heads + h, n_kv, lines), :] for s in range(seq)
            ]
            blocks.append(jnp.concatenate(parts, axis=0))
        halves.append(jnp.concatenate(blocks, axis=1))
    tp_at = lax.axis_index("tp")
    width = resid_ref.shape[1]
    cols = pl.ds(pl.multiple_of(tp_at * width, width), width)
    first = tp_at == 0
    own = jnp.where(first, halves[0], halves[1]).astype(BF)
    other = jnp.where(first, halves[1], halves[0]).astype(BF)
    mixed = dot(own, own_ref[:, cols]).astype(BF).astype(F32)
    mixed = mixed + dot(other, other_ref[:, cols]).astype(BF).astype(F32)
    for s in range(seq):
        mixed_ref[pl.ds(s, n_kv, seq), :] = mixed[s * n_kv : (s + 1) * n_kv]
    resid = (tokens_ref[...].astype(F32) + mixed_ref[...]).astype(BF)
    resid_ref[...] = resid
    for d in range(spread_ref.shape[0]):
        spread_ref[d] = resid


def feed_kernel(
    got_ref,
    gains_ref,
    up_ref,
    down_ref,
    state_ref,
    out_ref,
    new_ref,
    sems,
    *,
    gain_line,
    model,
    n_tp,
):
    copies = [
        pltpu.make_async_copy(state_ref.at[n, m], new_ref.at[n, m], sems.at[n, m])
        for n in range(state_ref.shape[0])
        for m in range(state_ref.shape[1])
    ]
    for copy in copies:
        copy.start()
    n_all, rows, width = got_ref.shape
    n_kv = n_all // n_tp
    lines = gains_ref.shape[0] // n_all
    squares = jnp.zeros((rows, width), F32)
    blocks = []
    for at in range(n_all):
        d = (at % n_tp) * n_kv + at // n_tp
        block = got_ref[d].astype(F32)
        squares = squares + block * block
        gain = gains_ref[d * lines : (d + 1) * lines].astype(F32)[gain_line : gain_line + 1]
        blocks.append((block * gain).astype(BF))
    inverse = lax.rsqrt(jnp.sum(squares, axis=1, keepdims=True) / model + 1e-06)
    scaled = jnp.concatenate(blocks, axis=1)
    up = jnp.dot(scaled, up_ref[...], preferred_element_type=F32) * inverse
    up = jnp.maximum(up, 0.0)
    act = (up * up).astype(BF)
    down = jnp.dot(act, down_ref[...], preferred_element_type=F32)
    for at in range(n_all):
        d = (at % n_tp) * n_kv + at // n_tp
        out_ref[d] = down[:, at * width : (at + 1) * width].astype(BF)
    for copy in copies:
        copy.wait()


def fused(
    tokens,
    state,
    mix_gain,
    w_query,
    w_key,
    w_value,
    w_beta,
    w_decay,
    decay_log,
    head_gain,
    w_out,
    ff_gain,
    w_up,
    w_down,
    n_kv,
    n_tp,
):
    rows, width = tokens.shape
    seq, heads, size = state.shape[:3]
    n_all = n_kv * n_tp
    model = width * n_all
    keys = heads * size
    per_seq = 3 * heads + 1
    packet = -(-seq * per_seq // 8) * 8
    lines = -(-(seq * heads + 1) // 8) * 8
    axes = ("tp", "kv")
    swap = [(i, n_tp - 1 - i) for i in range(n_tp)]
    shape = jax.ShapeDtypeStruct
    vmem = pl.BlockSpec(memory_space=pltpu.VMEM)
    cost = pl.CostEstimate(flops=4 * 10**9, bytes_accessed=8 * 10**6, transcendentals=0)
    params = pltpu.CompilerParams(vmem_limit_bytes=16 * 1024 * 1024)

    gain_row = mix_gain[None, :]
    other_tokens = lax.ppermute(tokens, "tp", swap)
    other_gain = lax.ppermute(gain_row, "tp", swap)
    hbm = pl.BlockSpec(memory_space=pltpu.HBM)
    other_out = lax.ppermute(w_out, "tp", swap)
    place = pl.pallas_call(
        place_kernel,
        out_shape=shape((LANES, 2 * heads), BF),
        out_specs=vmem,
        name="place",
        cost_estimate=cost,
        compiler_params=params,
    )()

    sent = pl.pallas_call(
        functools.partial(project_kernel, n_kv=n_kv, seq=seq, heads=heads),
        out_shape=shape((n_kv * packet, LANES), BF),
        in_specs=[vmem] * 10,
        out_specs=vmem,
        scratch_shapes=[
            pltpu.VMEM((per_seq * rows, LANES), F32),
            pltpu.VMEM((n_kv * packet, LANES), F32),
        ],
        name="project",
        cost_estimate=cost,
        compiler_params=params,
    )(
        place,
        tokens,
        gain_row,
        other_tokens,
        other_gain,
        w_query,
        w_key,
        w_value,
        w_beta.T,
        w_decay.T,
    )
    sent, other_out = lax.optimization_barrier((sent, other_out))
    got = lax.all_to_all(sent.reshape(n_kv, packet, LANES), "kv", 0, 0, tiled=False)
    spread, new_state = pl.pallas_call(
        functools.partial(delta_kernel, n_kv=n_kv, seq=seq, heads=heads, model=model),
        out_shape=(shape((n_all, lines, LANES), BF), shape(state.shape, F32)),
        in_specs=[vmem] * 5,
        out_specs=(vmem, vmem),
        name="delta",
        cost_estimate=cost,
        compiler_params=params,
    )(got.reshape(n_kv * packet, LANES), state, decay_log[None, :], head_gain[None, :], ff_gain[None, :])
    got = lax.all_to_all(spread, axes, 0, 0, tiled=False).reshape(n_all * lines, LANES)
    spread, resid = pl.pallas_call(
        functools.partial(mix_kernel, n_kv=n_kv, n_tp=n_tp, seq=seq, heads=heads),
        out_shape=(shape((n_all, rows, width), BF), shape((rows, width), BF)),
        in_specs=[vmem] * 4,
        out_specs=(vmem, vmem),
        scratch_shapes=[
            pltpu.VMEM((n_all * lines, LANES), F32),
            pltpu.VMEM((rows, width), F32),
        ],
        name="mix",
        cost_estimate=cost,
        compiler_params=params,
    )(got, tokens, w_out, other_out)
    got2 = lax.all_to_all(spread, axes, 0, 0, tiled=False)
    down, new_state = pl.pallas_call(
        functools.partial(feed_kernel, gain_line=seq * heads, model=model, n_tp=n_tp),
        out_shape=(shape((n_all, rows, width), BF), shape(state.shape, F32)),
        in_specs=[vmem] * 5,
        out_specs=(vmem, hbm),
        scratch_shapes=[pltpu.SemaphoreType.DMA((seq, heads))],
        name="feed",
        compiler_params=params,
    )(got2, got, w_up, w_down, new_state)
    got3 = lax.all_to_all(down, axes, 0, 0, tiled=False)
    output = (resid.astype(F32) + jnp.sum(got3.astype(F32), axis=0)).astype(BF)
    return (output, new_state)


def local(*arrays, n_kv, n_tp):
    tokens, state = arrays[:2]
    whole_tiles = tokens.shape[1] == LANES and state.shape[2] == LANES and n_kv % 8 == 0 and n_tp == 2
    form = fused if whole_tiles else plain
    return form(*arrays, n_kv=n_kv, n_tp=n_tp)


def solution(mesh):
    placed = (
        P("dp", ("kv", "tp")),
        P(("dp", "kv"), "tp", None, None),
        P(("kv", "tp")),
        P("kv", "tp"),
        P("kv", "tp"),
        P("kv", "tp"),
        P("kv", "tp"),
        P("kv", "tp"),
        P("tp"),
        P(),
        P("tp", "kv"),
        P(("kv", "tp")),
        P(None, ("kv", "tp")),
        P(("kv", "tp"), None),
    )
    return jax.shard_map(
        functools.partial(local, n_kv=mesh.shape["kv"], n_tp=mesh.shape["tp"]),
        mesh=mesh,
        in_specs=placed,
        out_specs=(P("dp", ("kv", "tp")), P(("dp", "kv"), "tp", None, None)),
        check_vma=False,
    )
```

```python
import functools

import jax
import jax.numpy as jnp
from jax import lax
from jax.experimental import pallas as pl
from jax.experimental.pallas import tpu as pltpu
from jax.sharding import PartitionSpec as P

BF = jnp.bfloat16
F32 = jnp.float32


def split_pair(value):
    high = value.astype(BF)
    low = (value - lax.reduce_precision(value, 8, 7)).astype(BF)
    return high, low


def plain(
    tokens,
    state,
    mix_gain,
    w_query,
    w_key,
    w_value,
    w_beta,
    w_decay,
    decay_log,
    head_gain,
    w_out,
    ff_gain,
    w_up,
    w_down,
    n_kv,
    n_tp,
):
    rows, width = tokens.shape
    seq, heads, size = state.shape[:3]
    n_all = n_kv * n_tp
    model = width * n_all
    keys = heads * size

    packed = jnp.concatenate([tokens, mix_gain[None, :]], axis=0)
    wide = lax.all_gather(packed, "tp", axis=1, tiled=True)
    tp_at = lax.axis_index("tp")
    out_cols = []
    for step in range(n_tp):
        target = (tp_at + step) % n_tp
        block = lax.dynamic_slice_in_dim(w_out, target * width, width, axis=1)
        if step:
            block = lax.ppermute(block, "tp", [(i, (i + step) % n_tp) for i in range(n_tp)])
        out_cols.append(block)

    wide_float = wide[:rows].astype(F32)
    scaled = (wide_float * wide[rows:].astype(F32)).astype(BF)
    dot = functools.partial(jnp.dot, preferred_element_type=F32)
    gates_part = dot(scaled, jnp.concatenate([w_beta, w_decay], axis=1))
    square_part = jnp.sum(wide_float * wide_float, axis=1, keepdims=True)
    small = jnp.concatenate([gates_part, square_part], axis=1)
    high, low = split_pair(small)
    n_small = small.shape[1]
    pad = jnp.zeros((rows, size - 2 * n_small), BF)
    sent = jnp.concatenate(
        [
            dot(scaled, w_query).astype(BF),
            dot(scaled, w_key).astype(BF),
            dot(scaled, w_value).astype(BF),
            high,
            low,
            pad,
        ],
        axis=1,
    ).reshape(n_kv, seq, 3 * keys + size)
    got = lax.all_to_all(sent, "kv", 0, 0, tiled=False)
    total = jnp.sum(got.astype(F32), axis=0)
    small = total[:, 3 * keys : 3 * keys + n_small] + total[:, 3 * keys + n_small : 3 * keys + 2 * n_small]
    inverse = lax.rsqrt(small[:, 2 * heads :] / model + 1e-06)
    query = (inverse * total[:, :keys]).reshape(seq, heads, size)
    key_rows = (inverse * total[:, keys : 2 * keys]).reshape(seq, heads, size)
    value = (inverse * total[:, 2 * keys : 3 * keys]).reshape(seq, heads, size)
    beta = jax.nn.sigmoid(inverse * small[:, :heads])
    decay = -jnp.exp(decay_log)[None, :] * jax.nn.softplus(inverse * small[:, heads : 2 * heads])
    qnorm = query * lax.rsqrt(jnp.sum(query * query, axis=-1, keepdims=True) + 1e-06)
    knorm = key_rows * lax.rsqrt(jnp.sum(key_rows * key_rows, axis=-1, keepdims=True) + 1e-06)
    kept = state * jnp.exp(decay)[:, :, None, None]
    predicted = jnp.sum(kept * knorm[:, :, :, None], axis=2)
    new_state = kept + (beta[:, :, None] * knorm)[:, :, :, None] * (value - predicted)[:, :, None, :]
    read = jnp.sum(new_state * qnorm[:, :, :, None], axis=2) / jnp.sqrt(jnp.float32(size))
    normed = (
        read
        * lax.rsqrt(jnp.mean(read * read, axis=-1, keepdims=True) + 1e-06)
        * head_gain.astype(F32)
    )
    normed = normed.astype(BF).reshape(seq, keys)
    axes = ("kv", "tp")
    spread = lax.all_to_all(jnp.broadcast_to(normed[None], (n_all, seq, keys)), axes, 0, 0, tiled=False)
    spread = spread.reshape(n_kv, n_tp, seq, keys)
    mixed = 0.0
    for step in range(n_tp):
        heads_of = lax.dynamic_index_in_dim(spread, (tp_at - step) % n_tp, 1, keepdims=False)
        part = dot(heads_of.reshape(rows, keys), out_cols[step])
        mixed = mixed + lax.reduce_precision(part, 8, 7)
    resid = (tokens.astype(F32) + mixed).astype(BF)
    resid_float = resid.astype(F32)
    scaled2 = (resid_float * ff_gain.astype(F32)[None, :]).astype(BF)
    high, low = split_pair(jnp.sum(resid_float * resid_float, axis=1))
    tail_rows = -(-2 * rows // width // 8) * 8
    tail = jnp.concatenate([high, low, jnp.zeros((tail_rows * width - 2 * rows,), BF)])
    tail = tail.reshape(tail_rows, width)
    sent2 = jnp.concatenate([scaled2, tail], axis=0)
    got2 = lax.all_to_all(jnp.broadcast_to(sent2[None], (n_all,) + sent2.shape), axes, 0, 0, tiled=False)
    sums = jnp.sum(got2[:, rows:].reshape(n_all, tail_rows * width)[:, : 2 * rows].astype(F32), axis=0)
    inverse2 = lax.rsqrt((sums[:rows] + sums[rows:]) / model + 1e-06)[:, None]
    whole = got2[:, :rows].transpose(1, 0, 2).reshape(rows, model)
    up_rows = dot(whole, w_up) * inverse2
    act = jnp.square(jax.nn.relu(up_rows)).astype(BF)
    down = dot(act, w_down).astype(BF).reshape(rows, n_all, width).transpose(1, 0, 2)
    got3 = lax.all_to_all(down, axes, 0, 0, tiled=False)
    output = (resid_float + jnp.sum(got3.astype(F32), axis=0)).astype(BF)
    return (output, new_state)


LANES = 128
SHIFT = 64


def place_kernel(out_ref):
    lane = lax.broadcasted_iota(jnp.int32, out_ref.shape, 0)
    head = lax.broadcasted_iota(jnp.int32, out_ref.shape, 1)
    out_ref[...] = jnp.where(lane == head, 1.0, 0.0).astype(BF)


def packet_line(s, j, seq, heads):
    if j < 2 * heads:
        return 2 * heads * s + j
    if j < 3 * heads:
        return 2 * heads * seq + heads * s + j - 2 * heads
    return 3 * heads * seq + s


def project_kernel(
    place_ref,
    own_ref,
    own_gain_ref,
    other_ref,
    other_gain_ref,
    wq_ref,
    wk_ref,
    wv_ref,
    wb_ref,
    wd_ref,
    out_ref,
    tokens_ref,
    pack_ref,
    *,
    n_kv,
    seq,
    heads,
):
    rows = own_ref.shape[0]
    first = lax.axis_index("tp") == 0
    own_rows = own_ref[...].astype(F32)
    other_rows = other_ref[...].astype(F32)
    tokens_ref[:rows, :] = jnp.where(first, own_rows, other_rows)
    tokens_ref[rows:, :] = jnp.where(first, other_rows, own_rows)
    own_gain = own_gain_ref[...].astype(F32)
    other_gain = other_gain_ref[...].astype(F32)
    gains = jnp.where(first, own_gain, other_gain), jnp.where(first, other_gain, own_gain)
    halves, squares = [], 0.0
    for t, gain in enumerate(gains):
        half = [tokens_ref[pl.ds(t * rows + s, n_kv, seq), :] for s in range(seq)]
        half = jnp.concatenate(half, axis=0)
        squares = squares + half * half
        halves.append((half * gain).astype(BF))
    squares = jnp.sum(squares, axis=1, keepdims=True)
    scaled = jnp.concatenate(halves, axis=1)
    dot = functools.partial(jnp.dot, preferred_element_type=F32)
    gate_weights = dot(place_ref[:, :heads], wb_ref[...])
    gate_weights = (gate_weights + dot(place_ref[:, heads:], wd_ref[...])).astype(BF)
    gates = lax.dot_general(
        scaled, gate_weights, (((1,), (1,)), ((), ())), preferred_element_type=F32
    )
    lanes = lax.broadcasted_iota(jnp.int32, (rows, LANES), 1)
    small = gates + jnp.where(lanes == 2 * heads, squares, 0.0)
    high = small.astype(BF).astype(F32)
    packet = out_ref.shape[0] // n_kv

    def pack(j, block):
        for s in range(seq):
            line = packet_line(s, j, seq, heads)
            pack_ref[pl.ds(line, n_kv, packet), :] = block[s * n_kv : (s + 1) * n_kv]

    for p, weight_ref in enumerate((wq_ref, wk_ref, wv_ref)):
        product = dot(scaled, weight_ref[...])
        for h in range(heads):
            pack(p * heads + h, product[:, h * LANES : (h + 1) * LANES])
    pack(3 * heads, high + pltpu.roll(small - high, SHIFT, 1))
    for j in range(seq * (3 * heads + 1), packet):
        pack_ref[pl.ds(j, n_kv, packet), :] = jnp.zeros((n_kv, LANES), F32)
    out_ref[...] = pack_ref[...].astype(BF)


def delta_kernel(
    got_ref,
    state_ref,
    decay_log_ref,
    head_gain_ref,
    ff_gain_ref,
    spread_ref,
    new_ref,
    *,
    n_kv,
    seq,
    heads,
    model,
):
    packet = got_ref.shape[0] // n_kv
    total = got_ref[:packet].astype(F32)
    for d in range(1, n_kv):
        total = total + got_ref[d * packet : (d + 1) * packet].astype(F32)
    pair = 2 * heads
    stack = total[: pair * seq]
    columns = stack.T
    lengths = jnp.sum(stack * stack, axis=1, keepdims=True)
    first = 3 * heads * seq
    start = first - first % 8
    small = total[start:]
    small = small + pltpu.roll(small, LANES - SHIFT, 1)
    inverses = lax.rsqrt(small[:, pair : pair + 1] / model + 1e-06)
    lane = lax.broadcasted_iota(jnp.int32, (1, LANES), 1)
    rate = jnp.zeros((1, LANES), F32)
    for h in range(heads):
        rate = jnp.where(lane == heads + h, decay_log_ref[:, h : h + 1], rate)
    gates = inverses * small
    betas = jax.nn.sigmoid(gates)
    soft = jnp.maximum(gates, 0.0) + jnp.log1p(jnp.exp(-jnp.abs(gates)))
    keeps = jnp.exp(-jnp.exp(rate) * soft)
    row = lax.broadcasted_iota(jnp.int32, (pair, LANES), 0)
    at_lane = lax.broadcasted_iota(jnp.int32, (pair, LANES), 1)
    head = jnp.where(row < heads, row, row - heads)
    reads = []
    for s in range(seq):
        line = first - start + s
        inverse = inverses[line : line + 1]
        beta = jnp.where(at_lane == head, betas[line : line + 1], 0.0)
        beta = jnp.sum(beta, axis=1, keepdims=True)
        keep = jnp.where(at_lane == head + heads, keeps[line : line + 1], 0.0)
        keep = jnp.sum(keep, axis=1, keepdims=True)
        vectors = stack[pair * s : pair * (s + 1)]
        length = lengths[pair * s : pair * (s + 1)]
        scale = inverse * lax.rsqrt(inverse * inverse * length + 1e-06)
        high = vectors.astype(BF)
        low = (vectors - high.astype(F32)).astype(BF)
        parts = jnp.concatenate([high, low], axis=0)
        found = jnp.zeros((pair, LANES), F32)
        for h in range(heads):
            block = state_ref[s, h]
            near = block.astype(BF)
            rest = (block - near.astype(F32)).astype(BF)
            both = jnp.dot(parts, near, preferred_element_type=F32)
            both = both + jnp.dot(parts, rest, preferred_element_type=F32)
            found = jnp.where(head == h, both[:pair] + both[pair:], found)
        found = found * (keep * scale)
        value = inverse * total[pair * seq + heads * s : pair * seq + heads * (s + 1)]
        change = (beta[:heads] * scale[heads:]) * (value - found[heads:])
        cross = jnp.sum(vectors[:heads] * vectors[heads:], axis=1, keepdims=True)
        reads.append(found[:heads] + (scale[:heads] * cross) * change)
        for h in range(heads):
            kcol = columns[:, pair * s + heads + h : pair * s + heads + h + 1]
            new_ref[s, h] = keep[h : h + 1] * state_ref[s, h] + kcol * change[h : h + 1]
    read = jnp.concatenate(reads, axis=0) / jnp.sqrt(jnp.float32(LANES))
    normed = (
        read
        * lax.rsqrt(jnp.mean(read * read, axis=1, keepdims=True) + 1e-06)
        * head_gain_ref[...].astype(F32)
    )
    lines = spread_ref.shape[1]
    fill = lines - seq * heads
    sent = jnp.concatenate(
        [normed, jnp.broadcast_to(ff_gain_ref[...].astype(F32), (fill, LANES))], axis=0
    ).astype(BF)
    for d in range(spread_ref.shape[0]):
        spread_ref[d] = sent


def mix_kernel(
    got_ref,
    tokens_ref,
    other_tokens_ref,
    own_ref,
    other_ref,
    spread_ref,
    resid_ref,
    rows_ref,
    mixed_ref,
    *,
    n_kv,
    n_tp,
    seq,
    heads,
):
    lines = got_ref.shape[0] // (n_kv * n_tp)
    rows, width = tokens_ref.shape
    rows_ref[...] = got_ref[...].astype(F32)
    dot = functools.partial(jnp.dot, preferred_element_type=F32)
    halves = []
    for t in range(n_tp):
        blocks = []
        for h in range(heads):
            parts = [
                rows_ref[pl.ds(t * n_kv * lines + s * heads + h, n_kv, lines), :] for s in range(seq)
            ]
            blocks.append(jnp.concatenate(parts, axis=0))
        halves.append(jnp.concatenate(blocks, axis=1))
    first = lax.axis_index("tp") == 0
    own = jnp.where(first, halves[0], halves[1]).astype(BF)
    other = jnp.where(first, halves[1], halves[0]).astype(BF)
    mixed = dot(own, own_ref[...]).astype(BF).astype(F32)
    mixed = mixed + dot(other, other_ref[...]).astype(BF).astype(F32)
    own_tokens = tokens_ref[...].astype(F32)
    other_tokens = other_tokens_ref[...].astype(F32)
    tokens = jnp.where(first, own_tokens, other_tokens), jnp.where(first, other_tokens, own_tokens)
    resids = []
    for t in range(n_tp):
        for s in range(seq):
            mixed_ref[pl.ds(t * rows + s, n_kv, seq), :] = mixed[
                s * n_kv : (s + 1) * n_kv, t * width : (t + 1) * width
            ]
        resids.append(tokens[t] + mixed_ref[t * rows : (t + 1) * rows, :])
    resid_ref[...] = jnp.where(first, resids[0], resids[1]).astype(BF)
    resid = jnp.concatenate(resids, axis=1).astype(BF)
    for d in range(n_kv):
        spread_ref[d] = resid


def feed_kernel(
    got_ref,
    gains_ref,
    up_ref,
    down_ref,
    state_ref,
    out_ref,
    new_ref,
    sems,
    *,
    gain_line,
    model,
    n_tp,
):
    copies = [
        pltpu.make_async_copy(state_ref.at[n, m], new_ref.at[n, m], sems.at[n, m])
        for n in range(state_ref.shape[0])
        for m in range(state_ref.shape[1])
    ]
    for copy in copies:
        copy.start()
    n_all, rows, width = out_ref.shape
    n_kv = n_all // n_tp
    lines = gains_ref.shape[0] // n_all
    squares = jnp.zeros((rows, n_tp * width), F32)
    blocks = []
    for d in range(n_kv):
        block = got_ref[d].astype(F32)
        squares = squares + block * block
        starts = [(t * n_kv + d) * lines for t in range(n_tp)]
        gain = [
            gains_ref[at : at + lines].astype(F32)[gain_line : gain_line + 1] for at in starts
        ]
        blocks.append((block * jnp.concatenate(gain, axis=1)).astype(BF))
    inverse = lax.rsqrt(jnp.sum(squares, axis=1, keepdims=True) / model + 1e-06)
    scaled = jnp.concatenate(blocks, axis=1)
    up = jnp.dot(scaled, up_ref[...], preferred_element_type=F32) * inverse
    up = jnp.maximum(up, 0.0)
    act = (up * up).astype(BF)
    down = jnp.dot(act, down_ref[...], preferred_element_type=F32)
    for at in range(n_all):
        d = (at % n_tp) * n_kv + at // n_tp
        out_ref[d] = down[:, at * width : (at + 1) * width].astype(BF)
    for copy in copies:
        copy.wait()


def fused(
    tokens,
    state,
    mix_gain,
    w_query,
    w_key,
    w_value,
    w_beta,
    w_decay,
    decay_log,
    head_gain,
    w_out,
    ff_gain,
    w_up,
    w_down,
    n_kv,
    n_tp,
):
    rows, width = tokens.shape
    seq, heads, size = state.shape[:3]
    n_all = n_kv * n_tp
    model = width * n_all
    keys = heads * size
    per_seq = 3 * heads + 1
    packet = -(-seq * per_seq // 8) * 8
    lines = -(-(seq * heads + 1) // 8) * 8
    axes = ("tp", "kv")
    swap = [(i, n_tp - 1 - i) for i in range(n_tp)]
    shape = jax.ShapeDtypeStruct
    vmem = pl.BlockSpec(memory_space=pltpu.VMEM)
    cost = pl.CostEstimate(flops=4 * 10**9, bytes_accessed=8 * 10**6, transcendentals=0)
    params = pltpu.CompilerParams(vmem_limit_bytes=16 * 1024 * 1024)

    gain_row = mix_gain[None, :]
    other_tokens = lax.ppermute(tokens, "tp", swap)
    other_gain = lax.ppermute(gain_row, "tp", swap)
    hbm = pl.BlockSpec(memory_space=pltpu.HBM)
    other_out = lax.ppermute(w_out, "tp", swap)
    place = pl.pallas_call(
        place_kernel,
        out_shape=shape((LANES, 2 * heads), BF),
        out_specs=vmem,
        name="place",
        cost_estimate=cost,
        compiler_params=params,
    )()

    sent = pl.pallas_call(
        functools.partial(project_kernel, n_kv=n_kv, seq=seq, heads=heads),
        out_shape=shape((n_kv * packet, LANES), BF),
        in_specs=[vmem] * 10,
        out_specs=vmem,
        scratch_shapes=[
            pltpu.VMEM((n_tp * rows, LANES), F32),
            pltpu.VMEM((n_kv * packet, LANES), F32),
        ],
        name="project",
        cost_estimate=cost,
        compiler_params=params,
    )(
        place,
        tokens,
        gain_row,
        other_tokens,
        other_gain,
        w_query,
        w_key,
        w_value,
        w_beta.T,
        w_decay.T,
    )
    sent, other_out = lax.optimization_barrier((sent, other_out))
    got = lax.all_to_all(sent.reshape(n_kv, packet, LANES), "kv", 0, 0, tiled=False)
    spread, new_state = pl.pallas_call(
        functools.partial(delta_kernel, n_kv=n_kv, seq=seq, heads=heads, model=model),
        out_shape=(shape((n_all, lines, LANES), BF), shape(state.shape, F32)),
        in_specs=[vmem] * 5,
        out_specs=(vmem, vmem),
        name="delta",
        cost_estimate=cost,
        compiler_params=params,
    )(got.reshape(n_kv * packet, LANES), state, decay_log[None, :], head_gain[None, :], ff_gain[None, :])
    got = lax.all_to_all(spread, axes, 0, 0, tiled=False).reshape(n_all * lines, LANES)
    spread, resid = pl.pallas_call(
        functools.partial(mix_kernel, n_kv=n_kv, n_tp=n_tp, seq=seq, heads=heads),
        out_shape=(shape((n_kv, rows, n_tp * width), BF), shape((rows, width), BF)),
        in_specs=[vmem] * 5,
        out_specs=(vmem, vmem),
        scratch_shapes=[
            pltpu.VMEM((n_all * lines, LANES), F32),
            pltpu.VMEM((n_tp * rows, width), F32),
        ],
        name="mix",
        cost_estimate=cost,
        compiler_params=params,
    )(got, tokens, other_tokens, w_out, other_out)
    got2 = lax.all_to_all(spread, "kv", 0, 0, tiled=False)
    down, new_state = pl.pallas_call(
        functools.partial(feed_kernel, gain_line=seq * heads, model=model, n_tp=n_tp),
        out_shape=(shape((n_all, rows, width), BF), shape(state.shape, F32)),
        in_specs=[vmem] * 5,
        out_specs=(vmem, hbm),
        scratch_shapes=[pltpu.SemaphoreType.DMA((seq, heads))],
        name="feed",
        compiler_params=params,
    )(got2, got, w_up, w_down, new_state)
    got3 = lax.all_to_all(down, axes, 0, 0, tiled=False)
    output = (resid.astype(F32) + jnp.sum(got3.astype(F32), axis=0)).astype(BF)
    return (output, new_state)


def local(*arrays, n_kv, n_tp):
    tokens, state = arrays[:2]
    whole_tiles = tokens.shape[1] == LANES and state.shape[2] == LANES and n_kv % 8 == 0 and n_tp == 2
    form = fused if whole_tiles else plain
    return form(*arrays, n_kv=n_kv, n_tp=n_tp)


def solution(mesh):
    placed = (
        P("dp", ("kv", "tp")),
        P(("dp", "kv"), "tp", None, None),
        P(("kv", "tp")),
        P("kv", "tp"),
        P("kv", "tp"),
        P("kv", "tp"),
        P("kv", "tp"),
        P("kv", "tp"),
        P("tp"),
        P(),
        P("tp", "kv"),
        P(("kv", "tp")),
        P(None, ("kv", "tp")),
        P(("kv", "tp"), None),
    )
    return jax.shard_map(
        functools.partial(local, n_kv=mesh.shape["kv"], n_tp=mesh.shape["tp"]),
        mesh=mesh,
        in_specs=placed,
        out_specs=(P("dp", ("kv", "tp")), P(("dp", "kv"), "tp", None, None)),
        check_vma=False,
    )
```

```python
import functools

import jax
import jax.numpy as jnp
from jax import lax
from jax.experimental import pallas as pl
from jax.experimental.pallas import tpu as pltpu
from jax.sharding import PartitionSpec as P

BF = jnp.bfloat16
F32 = jnp.float32


def split_pair(value):
    high = value.astype(BF)
    low = (value - lax.reduce_precision(value, 8, 7)).astype(BF)
    return high, low


def plain(
    tokens,
    state,
    mix_gain,
    w_query,
    w_key,
    w_value,
    w_beta,
    w_decay,
    decay_log,
    head_gain,
    w_out,
    ff_gain,
    w_up,
    w_down,
    n_kv,
    n_tp,
):
    rows, width = tokens.shape
    seq, heads, size = state.shape[:3]
    n_all = n_kv * n_tp
    model = width * n_all
    keys = heads * size

    packed = jnp.concatenate([tokens, mix_gain[None, :]], axis=0)
    wide = lax.all_gather(packed, "tp", axis=1, tiled=True)
    tp_at = lax.axis_index("tp")
    out_cols = []
    for step in range(n_tp):
        target = (tp_at + step) % n_tp
        block = lax.dynamic_slice_in_dim(w_out, target * width, width, axis=1)
        if step:
            block = lax.ppermute(block, "tp", [(i, (i + step) % n_tp) for i in range(n_tp)])
        out_cols.append(block)

    wide_float = wide[:rows].astype(F32)
    scaled = (wide_float * wide[rows:].astype(F32)).astype(BF)
    dot = functools.partial(jnp.dot, preferred_element_type=F32)
    gates_part = dot(scaled, jnp.concatenate([w_beta, w_decay], axis=1))
    square_part = jnp.sum(wide_float * wide_float, axis=1, keepdims=True)
    small = jnp.concatenate([gates_part, square_part], axis=1)
    high, low = split_pair(small)
    n_small = small.shape[1]
    pad = jnp.zeros((rows, size - 2 * n_small), BF)
    sent = jnp.concatenate(
        [
            dot(scaled, w_query).astype(BF),
            dot(scaled, w_key).astype(BF),
            dot(scaled, w_value).astype(BF),
            high,
            low,
            pad,
        ],
        axis=1,
    ).reshape(n_kv, seq, 3 * keys + size)
    got = lax.all_to_all(sent, "kv", 0, 0, tiled=False)
    total = jnp.sum(got.astype(F32), axis=0)
    small = total[:, 3 * keys : 3 * keys + n_small] + total[:, 3 * keys + n_small : 3 * keys + 2 * n_small]
    inverse = lax.rsqrt(small[:, 2 * heads :] / model + 1e-06)
    query = (inverse * total[:, :keys]).reshape(seq, heads, size)
    key_rows = (inverse * total[:, keys : 2 * keys]).reshape(seq, heads, size)
    value = (inverse * total[:, 2 * keys : 3 * keys]).reshape(seq, heads, size)
    beta = jax.nn.sigmoid(inverse * small[:, :heads])
    decay = -jnp.exp(decay_log)[None, :] * jax.nn.softplus(inverse * small[:, heads : 2 * heads])
    qnorm = query * lax.rsqrt(jnp.sum(query * query, axis=-1, keepdims=True) + 1e-06)
    knorm = key_rows * lax.rsqrt(jnp.sum(key_rows * key_rows, axis=-1, keepdims=True) + 1e-06)
    kept = state * jnp.exp(decay)[:, :, None, None]
    predicted = jnp.sum(kept * knorm[:, :, :, None], axis=2)
    new_state = kept + (beta[:, :, None] * knorm)[:, :, :, None] * (value - predicted)[:, :, None, :]
    read = jnp.sum(new_state * qnorm[:, :, :, None], axis=2) / jnp.sqrt(jnp.float32(size))
    normed = (
        read
        * lax.rsqrt(jnp.mean(read * read, axis=-1, keepdims=True) + 1e-06)
        * head_gain.astype(F32)
    )
    normed = normed.astype(BF).reshape(seq, keys)
    axes = ("kv", "tp")
    spread = lax.all_to_all(jnp.broadcast_to(normed[None], (n_all, seq, keys)), axes, 0, 0, tiled=False)
    spread = spread.reshape(n_kv, n_tp, seq, keys)
    mixed = 0.0
    for step in range(n_tp):
        heads_of = lax.dynamic_index_in_dim(spread, (tp_at - step) % n_tp, 1, keepdims=False)
        part = dot(heads_of.reshape(rows, keys), out_cols[step])
        mixed = mixed + lax.reduce_precision(part, 8, 7)
    resid = (tokens.astype(F32) + mixed).astype(BF)
    resid_float = resid.astype(F32)
    scaled2 = (resid_float * ff_gain.astype(F32)[None, :]).astype(BF)
    high, low = split_pair(jnp.sum(resid_float * resid_float, axis=1))
    tail_rows = -(-2 * rows // width // 8) * 8
    tail = jnp.concatenate([high, low, jnp.zeros((tail_rows * width - 2 * rows,), BF)])
    tail = tail.reshape(tail_rows, width)
    sent2 = jnp.concatenate([scaled2, tail], axis=0)
    got2 = lax.all_to_all(jnp.broadcast_to(sent2[None], (n_all,) + sent2.shape), axes, 0, 0, tiled=False)
    sums = jnp.sum(got2[:, rows:].reshape(n_all, tail_rows * width)[:, : 2 * rows].astype(F32), axis=0)
    inverse2 = lax.rsqrt((sums[:rows] + sums[rows:]) / model + 1e-06)[:, None]
    whole = got2[:, :rows].transpose(1, 0, 2).reshape(rows, model)
    up_rows = dot(whole, w_up) * inverse2
    act = jnp.square(jax.nn.relu(up_rows)).astype(BF)
    down = dot(act, w_down).astype(BF).reshape(rows, n_all, width).transpose(1, 0, 2)
    got3 = lax.all_to_all(down, axes, 0, 0, tiled=False)
    output = (resid_float + jnp.sum(got3.astype(F32), axis=0)).astype(BF)
    return (output, new_state)


LANES = 128
SHIFT = 64
ORDERS = {
    8: (4, 5, 6, 0, 7, 1, 3, 2),
    16: (11, 8, 13, 3, 9, 0, 15, 1, 10, 5, 6, 2, 12, 14, 7, 4),
}


def ring(count):
    return ORDERS.get(count, tuple(range(count)))


def exchange(blocks, axes):
    return lax.all_to_all(
        blocks, axes, 0, 0, tiled=False, axis_index_groups=[list(ring(blocks.shape[0]))]
    )


def place_kernel(out_ref):
    lane = lax.broadcasted_iota(jnp.int32, out_ref.shape, 0)
    head = lax.broadcasted_iota(jnp.int32, out_ref.shape, 1)
    out_ref[...] = jnp.where(lane == head, 1.0, 0.0).astype(BF)


def packet_line(s, j, seq, heads):
    if j < 2 * heads:
        return 2 * heads * s + j
    if j < 3 * heads:
        return 2 * heads * seq + heads * s + j - 2 * heads
    return 3 * heads * seq + s


def project_kernel(
    place_ref,
    own_ref,
    own_gain_ref,
    other_ref,
    other_gain_ref,
    wq_ref,
    wk_ref,
    wv_ref,
    wb_ref,
    wd_ref,
    out_ref,
    tokens_ref,
    pack_ref,
    *,
    n_kv,
    seq,
    heads,
):
    rows = own_ref.shape[0]
    first = lax.axis_index("tp") == 0
    own_rows = own_ref[...].astype(F32)
    other_rows = other_ref[...].astype(F32)
    tokens_ref[:rows, :] = jnp.where(first, own_rows, other_rows)
    tokens_ref[rows:, :] = jnp.where(first, other_rows, own_rows)
    own_gain = own_gain_ref[...].astype(F32)
    other_gain = other_gain_ref[...].astype(F32)
    gains = jnp.where(first, own_gain, other_gain), jnp.where(first, other_gain, own_gain)
    halves, squares = [], 0.0
    for t, gain in enumerate(gains):
        half = [tokens_ref[pl.ds(t * rows + s, n_kv, seq), :] for s in range(seq)]
        half = jnp.concatenate(half, axis=0)
        squares = squares + half * half
        halves.append((half * gain).astype(BF))
    squares = jnp.sum(squares, axis=1, keepdims=True)
    scaled = jnp.concatenate(halves, axis=1)
    dot = functools.partial(jnp.dot, preferred_element_type=F32)
    gate_weights = dot(place_ref[:, :heads], wb_ref[...])
    gate_weights = (gate_weights + dot(place_ref[:, heads:], wd_ref[...])).astype(BF)
    gates = lax.dot_general(
        scaled, gate_weights, (((1,), (1,)), ((), ())), preferred_element_type=F32
    )
    lanes = lax.broadcasted_iota(jnp.int32, (rows, LANES), 1)
    small = gates + jnp.where(lanes == 2 * heads, squares, 0.0)
    high = small.astype(BF).astype(F32)
    packet = out_ref.shape[0] // n_kv

    def pack(j, block):
        for s in range(seq):
            line = packet_line(s, j, seq, heads)
            pack_ref[pl.ds(line, n_kv, packet), :] = block[s * n_kv : (s + 1) * n_kv]

    for p, weight_ref in enumerate((wq_ref, wk_ref, wv_ref)):
        product = dot(scaled, weight_ref[...])
        for h in range(heads):
            pack(p * heads + h, product[:, h * LANES : (h + 1) * LANES])
    pack(3 * heads, high + pltpu.roll(small - high, SHIFT, 1))
    for j in range(seq * (3 * heads + 1), packet):
        pack_ref[pl.ds(j, n_kv, packet), :] = jnp.zeros((n_kv, LANES), F32)
    for k, d in enumerate(ring(n_kv)):
        out_ref[k * packet : (k + 1) * packet] = pack_ref[d * packet : (d + 1) * packet].astype(BF)


def delta_kernel(
    got_ref,
    state_ref,
    decay_log_ref,
    head_gain_ref,
    ff_gain_ref,
    spread_ref,
    new_ref,
    *,
    n_kv,
    seq,
    heads,
    model,
):
    packet = got_ref.shape[0] // n_kv
    total = got_ref[:packet].astype(F32)
    for d in range(1, n_kv):
        total = total + got_ref[d * packet : (d + 1) * packet].astype(F32)
    pair = 2 * heads
    stack = total[: pair * seq]
    columns = stack.T
    lengths = jnp.sum(stack * stack, axis=1, keepdims=True)
    first = 3 * heads * seq
    start = first - first % 8
    small = total[start:]
    small = small + pltpu.roll(small, LANES - SHIFT, 1)
    inverses = lax.rsqrt(small[:, pair : pair + 1] / model + 1e-06)
    lane = lax.broadcasted_iota(jnp.int32, (1, LANES), 1)
    rate = jnp.zeros((1, LANES), F32)
    for h in range(heads):
        rate = jnp.where(lane == heads + h, decay_log_ref[:, h : h + 1], rate)
    gates = inverses * small
    betas = jax.nn.sigmoid(gates)
    soft = jnp.maximum(gates, 0.0) + jnp.log1p(jnp.exp(-jnp.abs(gates)))
    keeps = jnp.exp(-jnp.exp(rate) * soft)
    row = lax.broadcasted_iota(jnp.int32, (pair, LANES), 0)
    at_lane = lax.broadcasted_iota(jnp.int32, (pair, LANES), 1)
    head = jnp.where(row < heads, row, row - heads)
    reads = []
    for s in range(seq):
        line = first - start + s
        inverse = inverses[line : line + 1]
        beta = jnp.where(at_lane == head, betas[line : line + 1], 0.0)
        beta = jnp.sum(beta, axis=1, keepdims=True)
        keep = jnp.where(at_lane == head + heads, keeps[line : line + 1], 0.0)
        keep = jnp.sum(keep, axis=1, keepdims=True)
        vectors = stack[pair * s : pair * (s + 1)]
        length = lengths[pair * s : pair * (s + 1)]
        scale = inverse * lax.rsqrt(inverse * inverse * length + 1e-06)
        high = vectors.astype(BF)
        low = (vectors - high.astype(F32)).astype(BF)
        parts = jnp.concatenate([high, low], axis=0)
        found = jnp.zeros((pair, LANES), F32)
        for h in range(heads):
            block = state_ref[s, h]
            near = block.astype(BF)
            rest = (block - near.astype(F32)).astype(BF)
            both = jnp.dot(parts, near, preferred_element_type=F32)
            both = both + jnp.dot(parts, rest, preferred_element_type=F32)
            found = jnp.where(head == h, both[:pair] + both[pair:], found)
        found = found * (keep * scale)
        value = inverse * total[pair * seq + heads * s : pair * seq + heads * (s + 1)]
        change = (beta[:heads] * scale[heads:]) * (value - found[heads:])
        cross = jnp.sum(vectors[:heads] * vectors[heads:], axis=1, keepdims=True)
        reads.append(found[:heads] + (scale[:heads] * cross) * change)
        for h in range(heads):
            kcol = columns[:, pair * s + heads + h : pair * s + heads + h + 1]
            new_ref[s, h] = keep[h : h + 1] * state_ref[s, h] + kcol * change[h : h + 1]
    read = jnp.concatenate(reads, axis=0) / jnp.sqrt(jnp.float32(LANES))
    normed = (
        read
        * lax.rsqrt(jnp.mean(read * read, axis=1, keepdims=True) + 1e-06)
        * head_gain_ref[...].astype(F32)
    )
    lines = spread_ref.shape[1]
    fill = lines - seq * heads
    sent = jnp.concatenate(
        [normed, jnp.broadcast_to(ff_gain_ref[...].astype(F32), (fill, LANES))], axis=0
    ).astype(BF)
    for d in range(spread_ref.shape[0]):
        spread_ref[d] = sent


def mix_kernel(
    got_ref,
    tokens_ref,
    other_tokens_ref,
    own_ref,
    other_ref,
    spread_ref,
    resid_ref,
    rows_ref,
    mixed_ref,
    *,
    n_kv,
    n_tp,
    seq,
    heads,
):
    lines = got_ref.shape[0] // (n_kv * n_tp)
    rows, width = tokens_ref.shape
    for k, member in enumerate(ring(n_kv * n_tp)):
        at = ((member % n_tp) * n_kv + member // n_tp) * lines
        rows_ref[at : at + lines] = got_ref[k * lines : (k + 1) * lines].astype(F32)
    dot = functools.partial(jnp.dot, preferred_element_type=F32)
    halves = []
    for t in range(n_tp):
        blocks = []
        for h in range(heads):
            parts = [
                rows_ref[pl.ds(t * n_kv * lines + s * heads + h, n_kv, lines), :] for s in range(seq)
            ]
            blocks.append(jnp.concatenate(parts, axis=0))
        halves.append(jnp.concatenate(blocks, axis=1))
    first = lax.axis_index("tp") == 0
    own = jnp.where(first, halves[0], halves[1]).astype(BF)
    other = jnp.where(first, halves[1], halves[0]).astype(BF)
    mixed = dot(own, own_ref[...]).astype(BF).astype(F32)
    mixed = mixed + dot(other, other_ref[...]).astype(BF).astype(F32)
    own_tokens = tokens_ref[...].astype(F32)
    other_tokens = other_tokens_ref[...].astype(F32)
    tokens = jnp.where(first, own_tokens, other_tokens), jnp.where(first, other_tokens, own_tokens)
    resids = []
    for t in range(n_tp):
        for s in range(seq):
            mixed_ref[pl.ds(t * rows + s, n_kv, seq), :] = mixed[
                s * n_kv : (s + 1) * n_kv, t * width : (t + 1) * width
            ]
        resids.append(tokens[t] + mixed_ref[t * rows : (t + 1) * rows, :])
    resid_ref[...] = jnp.where(first, resids[0], resids[1]).astype(BF)
    resid = jnp.concatenate(resids, axis=1).astype(BF)
    for d in range(n_kv):
        spread_ref[d] = resid


def feed_kernel(
    got_ref,
    gains_ref,
    up_ref,
    down_ref,
    state_ref,
    out_ref,
    new_ref,
    sems,
    *,
    gain_line,
    model,
    n_tp,
):
    copies = [
        pltpu.make_async_copy(state_ref.at[n, m], new_ref.at[n, m], sems.at[n, m])
        for n in range(state_ref.shape[0])
        for m in range(state_ref.shape[1])
    ]
    for copy in copies:
        copy.start()
    n_all, rows, width = out_ref.shape
    n_kv = n_all // n_tp
    lines = gains_ref.shape[0] // n_all
    squares = jnp.zeros((rows, n_tp * width), F32)
    blocks = []
    for d in range(n_kv):
        block = got_ref[ring(n_kv).index(d)].astype(F32)
        squares = squares + block * block
        starts = [ring(n_all).index(d * n_tp + t) * lines for t in range(n_tp)]
        gain = [
            gains_ref[at : at + lines].astype(F32)[gain_line : gain_line + 1] for at in starts
        ]
        blocks.append((block * jnp.concatenate(gain, axis=1)).astype(BF))
    inverse = lax.rsqrt(jnp.sum(squares, axis=1, keepdims=True) / model + 1e-06)
    scaled = jnp.concatenate(blocks, axis=1)
    up = jnp.dot(scaled, up_ref[...], preferred_element_type=F32) * inverse
    up = jnp.maximum(up, 0.0)
    act = (up * up).astype(BF)
    down = jnp.dot(act, down_ref[...], preferred_element_type=F32)
    for k, at in enumerate(ring(n_all)):
        out_ref[k] = down[:, at * width : (at + 1) * width].astype(BF)
    for copy in copies:
        copy.wait()


def fused(
    tokens,
    state,
    mix_gain,
    w_query,
    w_key,
    w_value,
    w_beta,
    w_decay,
    decay_log,
    head_gain,
    w_out,
    ff_gain,
    w_up,
    w_down,
    n_kv,
    n_tp,
):
    rows, width = tokens.shape
    seq, heads, size = state.shape[:3]
    n_all = n_kv * n_tp
    model = width * n_all
    keys = heads * size
    per_seq = 3 * heads + 1
    packet = -(-seq * per_seq // 8) * 8
    lines = -(-(seq * heads + 1) // 8) * 8
    axes = ("kv", "tp")
    swap = [(i, n_tp - 1 - i) for i in range(n_tp)]
    shape = jax.ShapeDtypeStruct
    vmem = pl.BlockSpec(memory_space=pltpu.VMEM)
    cost = pl.CostEstimate(flops=4 * 10**9, bytes_accessed=8 * 10**6, transcendentals=0)
    params = pltpu.CompilerParams(vmem_limit_bytes=16 * 1024 * 1024)

    gain_row = mix_gain[None, :]
    other_tokens = lax.ppermute(tokens, "tp", swap)
    other_gain = lax.ppermute(gain_row, "tp", swap)
    hbm = pl.BlockSpec(memory_space=pltpu.HBM)
    other_out = lax.ppermute(w_out, "tp", swap)
    place = pl.pallas_call(
        place_kernel,
        out_shape=shape((LANES, 2 * heads), BF),
        out_specs=vmem,
        name="place",
        cost_estimate=cost,
        compiler_params=params,
    )()

    sent = pl.pallas_call(
        functools.partial(project_kernel, n_kv=n_kv, seq=seq, heads=heads),
        out_shape=shape((n_kv * packet, LANES), BF),
        in_specs=[vmem] * 10,
        out_specs=vmem,
        scratch_shapes=[
            pltpu.VMEM((n_tp * rows, LANES), F32),
            pltpu.VMEM((n_kv * packet, LANES), F32),
        ],
        name="project",
        cost_estimate=cost,
        compiler_params=params,
    )(
        place,
        tokens,
        gain_row,
        other_tokens,
        other_gain,
        w_query,
        w_key,
        w_value,
        w_beta.T,
        w_decay.T,
    )
    sent, other_out = lax.optimization_barrier((sent, other_out))
    got = exchange(sent.reshape(n_kv, packet, LANES), "kv")
    spread, new_state = pl.pallas_call(
        functools.partial(delta_kernel, n_kv=n_kv, seq=seq, heads=heads, model=model),
        out_shape=(shape((n_all, lines, LANES), BF), shape(state.shape, F32)),
        in_specs=[vmem] * 5,
        out_specs=(vmem, vmem),
        name="delta",
        cost_estimate=cost,
        compiler_params=params,
    )(got.reshape(n_kv * packet, LANES), state, decay_log[None, :], head_gain[None, :], ff_gain[None, :])
    got = exchange(spread, axes).reshape(n_all * lines, LANES)
    spread, resid = pl.pallas_call(
        functools.partial(mix_kernel, n_kv=n_kv, n_tp=n_tp, seq=seq, heads=heads),
        out_shape=(shape((n_kv, rows, n_tp * width), BF), shape((rows, width), BF)),
        in_specs=[vmem] * 5,
        out_specs=(vmem, vmem),
        scratch_shapes=[
            pltpu.VMEM((n_all * lines, LANES), F32),
            pltpu.VMEM((n_tp * rows, width), F32),
        ],
        name="mix",
        cost_estimate=cost,
        compiler_params=params,
    )(got, tokens, other_tokens, w_out, other_out)
    got2 = exchange(spread, "kv")
    down, new_state = pl.pallas_call(
        functools.partial(feed_kernel, gain_line=seq * heads, model=model, n_tp=n_tp),
        out_shape=(shape((n_all, rows, width), BF), shape(state.shape, F32)),
        in_specs=[vmem] * 5,
        out_specs=(vmem, hbm),
        scratch_shapes=[pltpu.SemaphoreType.DMA((seq, heads))],
        name="feed",
        compiler_params=params,
    )(got2, got, w_up, w_down, new_state)
    got3 = exchange(down, axes)
    output = (resid.astype(F32) + jnp.sum(got3.astype(F32), axis=0)).astype(BF)
    return (output, new_state)


def local(*arrays, n_kv, n_tp):
    tokens, state = arrays[:2]
    whole_tiles = tokens.shape[1] == LANES and state.shape[2] == LANES and n_kv % 8 == 0 and n_tp == 2
    form = fused if whole_tiles else plain
    return form(*arrays, n_kv=n_kv, n_tp=n_tp)


def solution(mesh):
    placed = (
        P("dp", ("kv", "tp")),
        P(("dp", "kv"), "tp", None, None),
        P(("kv", "tp")),
        P("kv", "tp"),
        P("kv", "tp"),
        P("kv", "tp"),
        P("kv", "tp"),
        P("kv", "tp"),
        P("tp"),
        P(),
        P("tp", "kv"),
        P(("kv", "tp")),
        P(None, ("kv", "tp")),
        P(("kv", "tp"), None),
    )
    return jax.shard_map(
        functools.partial(local, n_kv=mesh.shape["kv"], n_tp=mesh.shape["tp"]),
        mesh=mesh,
        in_specs=placed,
        out_specs=(P("dp", ("kv", "tp")), P(("dp", "kv"), "tp", None, None)),
        check_vma=False,
    )
```

```python
import functools

import jax
import jax.numpy as jnp
from jax import lax
from jax.experimental import pallas as pl
from jax.experimental.pallas import tpu as pltpu
from jax.sharding import PartitionSpec as P

BF = jnp.bfloat16
F32 = jnp.float32


def split_pair(value):
    high = value.astype(BF)
    low = (value - lax.reduce_precision(value, 8, 7)).astype(BF)
    return high, low


def plain(
    tokens,
    state,
    mix_gain,
    w_query,
    w_key,
    w_value,
    w_beta,
    w_decay,
    decay_log,
    head_gain,
    w_out,
    ff_gain,
    w_up,
    w_down,
    n_kv,
    n_tp,
):
    rows, width = tokens.shape
    seq, heads, size = state.shape[:3]
    n_all = n_kv * n_tp
    model = width * n_all
    keys = heads * size

    packed = jnp.concatenate([tokens, mix_gain[None, :]], axis=0)
    wide = lax.all_gather(packed, "tp", axis=1, tiled=True)
    tp_at = lax.axis_index("tp")
    out_cols = []
    for step in range(n_tp):
        target = (tp_at + step) % n_tp
        block = lax.dynamic_slice_in_dim(w_out, target * width, width, axis=1)
        if step:
            block = lax.ppermute(block, "tp", [(i, (i + step) % n_tp) for i in range(n_tp)])
        out_cols.append(block)

    wide_float = wide[:rows].astype(F32)
    scaled = (wide_float * wide[rows:].astype(F32)).astype(BF)
    dot = functools.partial(jnp.dot, preferred_element_type=F32)
    gates_part = dot(scaled, jnp.concatenate([w_beta, w_decay], axis=1))
    square_part = jnp.sum(wide_float * wide_float, axis=1, keepdims=True)
    small = jnp.concatenate([gates_part, square_part], axis=1)
    high, low = split_pair(small)
    n_small = small.shape[1]
    pad = jnp.zeros((rows, size - 2 * n_small), BF)
    sent = jnp.concatenate(
        [
            dot(scaled, w_query).astype(BF),
            dot(scaled, w_key).astype(BF),
            dot(scaled, w_value).astype(BF),
            high,
            low,
            pad,
        ],
        axis=1,
    ).reshape(n_kv, seq, 3 * keys + size)
    got = lax.all_to_all(sent, "kv", 0, 0, tiled=False)
    total = jnp.sum(got.astype(F32), axis=0)
    small = total[:, 3 * keys : 3 * keys + n_small] + total[:, 3 * keys + n_small : 3 * keys + 2 * n_small]
    inverse = lax.rsqrt(small[:, 2 * heads :] / model + 1e-06)
    query = (inverse * total[:, :keys]).reshape(seq, heads, size)
    key_rows = (inverse * total[:, keys : 2 * keys]).reshape(seq, heads, size)
    value = (inverse * total[:, 2 * keys : 3 * keys]).reshape(seq, heads, size)
    beta = jax.nn.sigmoid(inverse * small[:, :heads])
    decay = -jnp.exp(decay_log)[None, :] * jax.nn.softplus(inverse * small[:, heads : 2 * heads])
    qnorm = query * lax.rsqrt(jnp.sum(query * query, axis=-1, keepdims=True) + 1e-06)
    knorm = key_rows * lax.rsqrt(jnp.sum(key_rows * key_rows, axis=-1, keepdims=True) + 1e-06)
    kept = state * jnp.exp(decay)[:, :, None, None]
    predicted = jnp.sum(kept * knorm[:, :, :, None], axis=2)
    new_state = kept + (beta[:, :, None] * knorm)[:, :, :, None] * (value - predicted)[:, :, None, :]
    read = jnp.sum(new_state * qnorm[:, :, :, None], axis=2) / jnp.sqrt(jnp.float32(size))
    normed = (
        read
        * lax.rsqrt(jnp.mean(read * read, axis=-1, keepdims=True) + 1e-06)
        * head_gain.astype(F32)
    )
    normed = normed.astype(BF).reshape(seq, keys)
    axes = ("kv", "tp")
    spread = lax.all_to_all(jnp.broadcast_to(normed[None], (n_all, seq, keys)), axes, 0, 0, tiled=False)
    spread = spread.reshape(n_kv, n_tp, seq, keys)
    mixed = 0.0
    for step in range(n_tp):
        heads_of = lax.dynamic_index_in_dim(spread, (tp_at - step) % n_tp, 1, keepdims=False)
        part = dot(heads_of.reshape(rows, keys), out_cols[step])
        mixed = mixed + lax.reduce_precision(part, 8, 7)
    resid = (tokens.astype(F32) + mixed).astype(BF)
    resid_float = resid.astype(F32)
    scaled2 = (resid_float * ff_gain.astype(F32)[None, :]).astype(BF)
    high, low = split_pair(jnp.sum(resid_float * resid_float, axis=1))
    tail_rows = -(-2 * rows // width // 8) * 8
    tail = jnp.concatenate([high, low, jnp.zeros((tail_rows * width - 2 * rows,), BF)])
    tail = tail.reshape(tail_rows, width)
    sent2 = jnp.concatenate([scaled2, tail], axis=0)
    got2 = lax.all_to_all(jnp.broadcast_to(sent2[None], (n_all,) + sent2.shape), axes, 0, 0, tiled=False)
    sums = jnp.sum(got2[:, rows:].reshape(n_all, tail_rows * width)[:, : 2 * rows].astype(F32), axis=0)
    inverse2 = lax.rsqrt((sums[:rows] + sums[rows:]) / model + 1e-06)[:, None]
    whole = got2[:, :rows].transpose(1, 0, 2).reshape(rows, model)
    up_rows = dot(whole, w_up) * inverse2
    act = jnp.square(jax.nn.relu(up_rows)).astype(BF)
    down = dot(act, w_down).astype(BF).reshape(rows, n_all, width).transpose(1, 0, 2)
    got3 = lax.all_to_all(down, axes, 0, 0, tiled=False)
    output = (resid_float + jnp.sum(got3.astype(F32), axis=0)).astype(BF)
    return (output, new_state)


LANES = 128
SHIFT = 64
ORDERS = {
    8: (5, 7, 6, 4, 3, 1, 2, 0),
    16: (11, 8, 13, 3, 9, 0, 15, 1, 10, 5, 6, 2, 12, 14, 7, 4),
}


FIRST = {8: (5, 7, 6, 4, 3, 1, 2, 0)}


def ring(count, first=False):
    return (FIRST if first else ORDERS).get(count, tuple(range(count)))


def exchange(blocks, axes, first=False):
    group = list(ring(blocks.shape[0], first))
    return lax.all_to_all(blocks, axes, 0, 0, tiled=False, axis_index_groups=[group])


def place_kernel(out_ref):
    lane = lax.broadcasted_iota(jnp.int32, out_ref.shape, 0)
    head = lax.broadcasted_iota(jnp.int32, out_ref.shape, 1)
    out_ref[...] = jnp.where(lane == head, 1.0, 0.0).astype(BF)


def packet_line(s, j, seq, heads):
    if j < 2 * heads:
        return 2 * heads * s + j
    if j < 3 * heads:
        return 2 * heads * seq + heads * s + j - 2 * heads
    return 3 * heads * seq + s


def project_kernel(
    place_ref,
    own_ref,
    own_gain_ref,
    other_ref,
    other_gain_ref,
    wq_ref,
    wk_ref,
    wv_ref,
    wb_ref,
    wd_ref,
    out_ref,
    tokens_ref,
    pack_ref,
    *,
    n_kv,
    seq,
    heads,
):
    rows = own_ref.shape[0]
    first = lax.axis_index("tp") == 0
    own_rows = own_ref[...].astype(F32)
    other_rows = other_ref[...].astype(F32)
    tokens_ref[:rows, :] = jnp.where(first, own_rows, other_rows)
    tokens_ref[rows:, :] = jnp.where(first, other_rows, own_rows)
    own_gain = own_gain_ref[...].astype(F32)
    other_gain = other_gain_ref[...].astype(F32)
    gains = jnp.where(first, own_gain, other_gain), jnp.where(first, other_gain, own_gain)
    halves, squares = [], 0.0
    for t, gain in enumerate(gains):
        half = [tokens_ref[pl.ds(t * rows + s, n_kv, seq), :] for s in range(seq)]
        half = jnp.concatenate(half, axis=0)
        squares = squares + half * half
        halves.append((half * gain).astype(BF))
    squares = jnp.sum(squares, axis=1, keepdims=True)
    scaled = jnp.concatenate(halves, axis=1)
    dot = functools.partial(jnp.dot, preferred_element_type=F32)
    gate_weights = dot(place_ref[:, :heads], wb_ref[...])
    gate_weights = (gate_weights + dot(place_ref[:, heads:], wd_ref[...])).astype(BF)
    gates = lax.dot_general(
        scaled, gate_weights, (((1,), (1,)), ((), ())), preferred_element_type=F32
    )
    lanes = lax.broadcasted_iota(jnp.int32, (rows, LANES), 1)
    small = gates + jnp.where(lanes == 2 * heads, squares, 0.0)
    high = small.astype(BF).astype(F32)
    packet = out_ref.shape[0] // n_kv

    def pack(j, block):
        for s in range(seq):
            line = packet_line(s, j, seq, heads)
            pack_ref[pl.ds(line, n_kv, packet), :] = block[s * n_kv : (s + 1) * n_kv]

    for p, weight_ref in enumerate((wq_ref, wk_ref, wv_ref)):
        product = dot(scaled, weight_ref[...])
        for h in range(heads):
            pack(p * heads + h, product[:, h * LANES : (h + 1) * LANES])
    pack(3 * heads, high + pltpu.roll(small - high, SHIFT, 1))
    for j in range(seq * (3 * heads + 1), packet):
        pack_ref[pl.ds(j, n_kv, packet), :] = jnp.zeros((n_kv, LANES), F32)
    for k, d in enumerate(ring(n_kv, True)):
        out_ref[k * packet : (k + 1) * packet] = pack_ref[d * packet : (d + 1) * packet].astype(BF)


def delta_kernel(
    got_ref,
    state_ref,
    decay_log_ref,
    head_gain_ref,
    ff_gain_ref,
    spread_ref,
    new_ref,
    *,
    n_kv,
    seq,
    heads,
    model,
):
    packet = got_ref.shape[0] // n_kv
    total = got_ref[:packet].astype(F32)
    for d in range(1, n_kv):
        total = total + got_ref[d * packet : (d + 1) * packet].astype(F32)
    pair = 2 * heads
    stack = total[: pair * seq]
    columns = stack.T
    lengths = jnp.sum(stack * stack, axis=1, keepdims=True)
    first = 3 * heads * seq
    start = first - first % 8
    small = total[start:]
    small = small + pltpu.roll(small, LANES - SHIFT, 1)
    inverses = lax.rsqrt(small[:, pair : pair + 1] / model + 1e-06)
    lane = lax.broadcasted_iota(jnp.int32, (1, LANES), 1)
    rate = jnp.zeros((1, LANES), F32)
    for h in range(heads):
        rate = jnp.where(lane == heads + h, decay_log_ref[:, h : h + 1], rate)
    gates = inverses * small
    betas = jax.nn.sigmoid(gates)
    soft = jnp.maximum(gates, 0.0) + jnp.log1p(jnp.exp(-jnp.abs(gates)))
    keeps = jnp.exp(-jnp.exp(rate) * soft)
    row = lax.broadcasted_iota(jnp.int32, (pair, LANES), 0)
    at_lane = lax.broadcasted_iota(jnp.int32, (pair, LANES), 1)
    head = jnp.where(row < heads, row, row - heads)
    reads = []
    for s in range(seq):
        line = first - start + s
        inverse = inverses[line : line + 1]
        beta = jnp.where(at_lane == head, betas[line : line + 1], 0.0)
        beta = jnp.sum(beta, axis=1, keepdims=True)
        keep = jnp.where(at_lane == head + heads, keeps[line : line + 1], 0.0)
        keep = jnp.sum(keep, axis=1, keepdims=True)
        vectors = stack[pair * s : pair * (s + 1)]
        length = lengths[pair * s : pair * (s + 1)]
        scale = inverse * lax.rsqrt(inverse * inverse * length + 1e-06)
        high = vectors.astype(BF)
        low = (vectors - high.astype(F32)).astype(BF)
        parts = jnp.concatenate([high, low], axis=0)
        found = jnp.zeros((pair, LANES), F32)
        for h in range(heads):
            block = state_ref[s, h]
            near = block.astype(BF)
            rest = (block - near.astype(F32)).astype(BF)
            both = jnp.dot(parts, near, preferred_element_type=F32)
            both = both + jnp.dot(parts, rest, preferred_element_type=F32)
            found = jnp.where(head == h, both[:pair] + both[pair:], found)
        found = found * (keep * scale)
        value = inverse * total[pair * seq + heads * s : pair * seq + heads * (s + 1)]
        change = (beta[:heads] * scale[heads:]) * (value - found[heads:])
        cross = jnp.sum(vectors[:heads] * vectors[heads:], axis=1, keepdims=True)
        reads.append(found[:heads] + (scale[:heads] * cross) * change)
        for h in range(heads):
            kcol = columns[:, pair * s + heads + h : pair * s + heads + h + 1]
            new_ref[s, h] = keep[h : h + 1] * state_ref[s, h] + kcol * change[h : h + 1]
    read = jnp.concatenate(reads, axis=0) / jnp.sqrt(jnp.float32(LANES))
    normed = (
        read
        * lax.rsqrt(jnp.mean(read * read, axis=1, keepdims=True) + 1e-06)
        * head_gain_ref[...].astype(F32)
    )
    lines = spread_ref.shape[1]
    fill = lines - seq * heads
    sent = jnp.concatenate(
        [normed, jnp.broadcast_to(ff_gain_ref[...].astype(F32), (fill, LANES))], axis=0
    ).astype(BF)
    for d in range(spread_ref.shape[0]):
        spread_ref[d] = sent


def mix_kernel(
    got_ref,
    tokens_ref,
    other_tokens_ref,
    own_ref,
    other_ref,
    spread_ref,
    resid_ref,
    rows_ref,
    mixed_ref,
    *,
    n_kv,
    n_tp,
    seq,
    heads,
):
    lines = got_ref.shape[0] // (n_kv * n_tp)
    rows, width = tokens_ref.shape
    for k, member in enumerate(ring(n_kv * n_tp)):
        at = ((member % n_tp) * n_kv + member // n_tp) * lines
        rows_ref[at : at + lines] = got_ref[k * lines : (k + 1) * lines].astype(F32)
    dot = functools.partial(jnp.dot, preferred_element_type=F32)
    halves = []
    for t in range(n_tp):
        blocks = []
        for h in range(heads):
            parts = [
                rows_ref[pl.ds(t * n_kv * lines + s * heads + h, n_kv, lines), :] for s in range(seq)
            ]
            blocks.append(jnp.concatenate(parts, axis=0))
        halves.append(jnp.concatenate(blocks, axis=1))
    first = lax.axis_index("tp") == 0
    own = jnp.where(first, halves[0], halves[1]).astype(BF)
    other = jnp.where(first, halves[1], halves[0]).astype(BF)
    mixed = dot(own, own_ref[...]).astype(BF).astype(F32)
    mixed = mixed + dot(other, other_ref[...]).astype(BF).astype(F32)
    own_tokens = tokens_ref[...].astype(F32)
    other_tokens = other_tokens_ref[...].astype(F32)
    tokens = jnp.where(first, own_tokens, other_tokens), jnp.where(first, other_tokens, own_tokens)
    resids = []
    for t in range(n_tp):
        for s in range(seq):
            mixed_ref[pl.ds(t * rows + s, n_kv, seq), :] = mixed[
                s * n_kv : (s + 1) * n_kv, t * width : (t + 1) * width
            ]
        resids.append(tokens[t] + mixed_ref[t * rows : (t + 1) * rows, :])
    resid_ref[...] = jnp.where(first, resids[0], resids[1]).astype(BF)
    resid = jnp.concatenate(resids, axis=1).astype(BF)
    for d in range(n_kv):
        spread_ref[d] = resid


def feed_kernel(
    got_ref,
    gains_ref,
    up_ref,
    down_ref,
    state_ref,
    out_ref,
    new_ref,
    sems,
    *,
    gain_line,
    model,
    n_tp,
):
    copies = [
        pltpu.make_async_copy(state_ref.at[n, m], new_ref.at[n, m], sems.at[n, m])
        for n in range(state_ref.shape[0])
        for m in range(state_ref.shape[1])
    ]
    for copy in copies:
        copy.start()
    n_all, rows, width = out_ref.shape
    n_kv = n_all // n_tp
    lines = gains_ref.shape[0] // n_all
    squares = jnp.zeros((rows, n_tp * width), F32)
    blocks = []
    for d in range(n_kv):
        block = got_ref[ring(n_kv).index(d)].astype(F32)
        squares = squares + block * block
        starts = [ring(n_all).index(d * n_tp + t) * lines for t in range(n_tp)]
        gain = [
            gains_ref[at : at + lines].astype(F32)[gain_line : gain_line + 1] for at in starts
        ]
        blocks.append((block * jnp.concatenate(gain, axis=1)).astype(BF))
    inverse = lax.rsqrt(jnp.sum(squares, axis=1, keepdims=True) / model + 1e-06)
    scaled = jnp.concatenate(blocks, axis=1)
    up = jnp.dot(scaled, up_ref[...], preferred_element_type=F32) * inverse
    up = jnp.maximum(up, 0.0)
    act = (up * up).astype(BF)
    down = jnp.dot(act, down_ref[...], preferred_element_type=F32)
    for k, at in enumerate(ring(n_all)):
        out_ref[k] = down[:, at * width : (at + 1) * width].astype(BF)
    for copy in copies:
        copy.wait()


def fused(
    tokens,
    state,
    mix_gain,
    w_query,
    w_key,
    w_value,
    w_beta,
    w_decay,
    decay_log,
    head_gain,
    w_out,
    ff_gain,
    w_up,
    w_down,
    n_kv,
    n_tp,
):
    rows, width = tokens.shape
    seq, heads, size = state.shape[:3]
    n_all = n_kv * n_tp
    model = width * n_all
    keys = heads * size
    per_seq = 3 * heads + 1
    packet = -(-seq * per_seq // 8) * 8
    lines = -(-(seq * heads + 1) // 8) * 8
    axes = ("kv", "tp")
    swap = [(i, n_tp - 1 - i) for i in range(n_tp)]
    shape = jax.ShapeDtypeStruct
    vmem = pl.BlockSpec(memory_space=pltpu.VMEM)
    cost = pl.CostEstimate(flops=4 * 10**9, bytes_accessed=8 * 10**6, transcendentals=0)
    params = pltpu.CompilerParams(vmem_limit_bytes=16 * 1024 * 1024)

    gain_row = mix_gain[None, :]
    other_tokens = lax.ppermute(tokens, "tp", swap)
    other_gain = lax.ppermute(gain_row, "tp", swap)
    hbm = pl.BlockSpec(memory_space=pltpu.HBM)
    other_out = lax.ppermute(w_out, "tp", swap)
    place = pl.pallas_call(
        place_kernel,
        out_shape=shape((LANES, 2 * heads), BF),
        out_specs=vmem,
        name="place",
        cost_estimate=cost,
        compiler_params=params,
    )()

    sent = pl.pallas_call(
        functools.partial(project_kernel, n_kv=n_kv, seq=seq, heads=heads),
        out_shape=shape((n_kv * packet, LANES), BF),
        in_specs=[vmem] * 10,
        out_specs=vmem,
        scratch_shapes=[
            pltpu.VMEM((n_tp * rows, LANES), F32),
            pltpu.VMEM((n_kv * packet, LANES), F32),
        ],
        name="project",
        cost_estimate=cost,
        compiler_params=params,
    )(
        place,
        tokens,
        gain_row,
        other_tokens,
        other_gain,
        w_query,
        w_key,
        w_value,
        w_beta.T,
        w_decay.T,
    )
    sent, other_out = lax.optimization_barrier((sent, other_out))
    got = exchange(sent.reshape(n_kv, packet, LANES), "kv", True)
    spread, new_state = pl.pallas_call(
        functools.partial(delta_kernel, n_kv=n_kv, seq=seq, heads=heads, model=model),
        out_shape=(shape((n_all, lines, LANES), BF), shape(state.shape, F32)),
        in_specs=[vmem] * 5,
        out_specs=(vmem, vmem),
        name="delta",
        cost_estimate=cost,
        compiler_params=params,
    )(got.reshape(n_kv * packet, LANES), state, decay_log[None, :], head_gain[None, :], ff_gain[None, :])
    got = exchange(spread, axes).reshape(n_all * lines, LANES)
    spread, resid = pl.pallas_call(
        functools.partial(mix_kernel, n_kv=n_kv, n_tp=n_tp, seq=seq, heads=heads),
        out_shape=(shape((n_kv, rows, n_tp * width), BF), shape((rows, width), BF)),
        in_specs=[vmem] * 5,
        out_specs=(vmem, vmem),
        scratch_shapes=[
            pltpu.VMEM((n_all * lines, LANES), F32),
            pltpu.VMEM((n_tp * rows, width), F32),
        ],
        name="mix",
        cost_estimate=cost,
        compiler_params=params,
    )(got, tokens, other_tokens, w_out, other_out)
    got2 = exchange(spread, "kv")
    down, new_state = pl.pallas_call(
        functools.partial(feed_kernel, gain_line=seq * heads, model=model, n_tp=n_tp),
        out_shape=(shape((n_all, rows, width), BF), shape(state.shape, F32)),
        in_specs=[vmem] * 5,
        out_specs=(vmem, hbm),
        scratch_shapes=[pltpu.SemaphoreType.DMA((seq, heads))],
        name="feed",
        compiler_params=params,
    )(got2, got, w_up, w_down, new_state)
    got3 = exchange(down, axes)
    output = (resid.astype(F32) + jnp.sum(got3.astype(F32), axis=0)).astype(BF)
    return (output, new_state)


def local(*arrays, n_kv, n_tp):
    tokens, state = arrays[:2]
    whole_tiles = tokens.shape[1] == LANES and state.shape[2] == LANES and n_kv % 8 == 0 and n_tp == 2
    form = fused if whole_tiles else plain
    return form(*arrays, n_kv=n_kv, n_tp=n_tp)


def solution(mesh):
    placed = (
        P("dp", ("kv", "tp")),
        P(("dp", "kv"), "tp", None, None),
        P(("kv", "tp")),
        P("kv", "tp"),
        P("kv", "tp"),
        P("kv", "tp"),
        P("kv", "tp"),
        P("kv", "tp"),
        P("tp"),
        P(),
        P("tp", "kv"),
        P(("kv", "tp")),
        P(None, ("kv", "tp")),
        P(("kv", "tp"), None),
    )
    return jax.shard_map(
        functools.partial(local, n_kv=mesh.shape["kv"], n_tp=mesh.shape["tp"]),
        mesh=mesh,
        in_specs=placed,
        out_specs=(P("dp", ("kv", "tp")), P(("dp", "kv"), "tp", None, None)),
        check_vma=False,
    )
```

```python
import functools

import jax
import jax.numpy as jnp
from jax import lax
from jax.experimental import pallas as pl
from jax.experimental.pallas import tpu as pltpu
from jax.sharding import PartitionSpec as P

BF = jnp.bfloat16
F32 = jnp.float32


def split_pair(value):
    high = value.astype(BF)
    low = (value - lax.reduce_precision(value, 8, 7)).astype(BF)
    return high, low


def plain(
    tokens,
    state,
    mix_gain,
    w_query,
    w_key,
    w_value,
    w_beta,
    w_decay,
    decay_log,
    head_gain,
    w_out,
    ff_gain,
    w_up,
    w_down,
    n_kv,
    n_tp,
):
    rows, width = tokens.shape
    seq, heads, size = state.shape[:3]
    n_all = n_kv * n_tp
    model = width * n_all
    keys = heads * size

    packed = jnp.concatenate([tokens, mix_gain[None, :]], axis=0)
    wide = lax.all_gather(packed, "tp", axis=1, tiled=True)
    tp_at = lax.axis_index("tp")
    out_cols = []
    for step in range(n_tp):
        target = (tp_at + step) % n_tp
        block = lax.dynamic_slice_in_dim(w_out, target * width, width, axis=1)
        if step:
            block = lax.ppermute(block, "tp", [(i, (i + step) % n_tp) for i in range(n_tp)])
        out_cols.append(block)

    wide_float = wide[:rows].astype(F32)
    scaled = (wide_float * wide[rows:].astype(F32)).astype(BF)
    dot = functools.partial(jnp.dot, preferred_element_type=F32)
    gates_part = dot(scaled, jnp.concatenate([w_beta, w_decay], axis=1))
    square_part = jnp.sum(wide_float * wide_float, axis=1, keepdims=True)
    small = jnp.concatenate([gates_part, square_part], axis=1)
    high, low = split_pair(small)
    n_small = small.shape[1]
    pad = jnp.zeros((rows, size - 2 * n_small), BF)
    sent = jnp.concatenate(
        [
            dot(scaled, w_query).astype(BF),
            dot(scaled, w_key).astype(BF),
            dot(scaled, w_value).astype(BF),
            high,
            low,
            pad,
        ],
        axis=1,
    ).reshape(n_kv, seq, 3 * keys + size)
    got = lax.all_to_all(sent, "kv", 0, 0, tiled=False)
    total = jnp.sum(got.astype(F32), axis=0)
    small = total[:, 3 * keys : 3 * keys + n_small] + total[:, 3 * keys + n_small : 3 * keys + 2 * n_small]
    inverse = lax.rsqrt(small[:, 2 * heads :] / model + 1e-06)
    query = (inverse * total[:, :keys]).reshape(seq, heads, size)
    key_rows = (inverse * total[:, keys : 2 * keys]).reshape(seq, heads, size)
    value = (inverse * total[:, 2 * keys : 3 * keys]).reshape(seq, heads, size)
    beta = jax.nn.sigmoid(inverse * small[:, :heads])
    decay = -jnp.exp(decay_log)[None, :] * jax.nn.softplus(inverse * small[:, heads : 2 * heads])
    qnorm = query * lax.rsqrt(jnp.sum(query * query, axis=-1, keepdims=True) + 1e-06)
    knorm = key_rows * lax.rsqrt(jnp.sum(key_rows * key_rows, axis=-1, keepdims=True) + 1e-06)
    kept = state * jnp.exp(decay)[:, :, None, None]
    predicted = jnp.sum(kept * knorm[:, :, :, None], axis=2)
    new_state = kept + (beta[:, :, None] * knorm)[:, :, :, None] * (value - predicted)[:, :, None, :]
    read = jnp.sum(new_state * qnorm[:, :, :, None], axis=2) / jnp.sqrt(jnp.float32(size))
    normed = (
        read
        * lax.rsqrt(jnp.mean(read * read, axis=-1, keepdims=True) + 1e-06)
        * head_gain.astype(F32)
    )
    normed = normed.astype(BF).reshape(seq, keys)
    axes = ("kv", "tp")
    spread = lax.all_to_all(jnp.broadcast_to(normed[None], (n_all, seq, keys)), axes, 0, 0, tiled=False)
    spread = spread.reshape(n_kv, n_tp, seq, keys)
    mixed = 0.0
    for step in range(n_tp):
        heads_of = lax.dynamic_index_in_dim(spread, (tp_at - step) % n_tp, 1, keepdims=False)
        part = dot(heads_of.reshape(rows, keys), out_cols[step])
        mixed = mixed + lax.reduce_precision(part, 8, 7)
    resid = (tokens.astype(F32) + mixed).astype(BF)
    resid_float = resid.astype(F32)
    scaled2 = (resid_float * ff_gain.astype(F32)[None, :]).astype(BF)
    high, low = split_pair(jnp.sum(resid_float * resid_float, axis=1))
    tail_rows = -(-2 * rows // width // 8) * 8
    tail = jnp.concatenate([high, low, jnp.zeros((tail_rows * width - 2 * rows,), BF)])
    tail = tail.reshape(tail_rows, width)
    sent2 = jnp.concatenate([scaled2, tail], axis=0)
    got2 = lax.all_to_all(jnp.broadcast_to(sent2[None], (n_all,) + sent2.shape), axes, 0, 0, tiled=False)
    sums = jnp.sum(got2[:, rows:].reshape(n_all, tail_rows * width)[:, : 2 * rows].astype(F32), axis=0)
    inverse2 = lax.rsqrt((sums[:rows] + sums[rows:]) / model + 1e-06)[:, None]
    whole = got2[:, :rows].transpose(1, 0, 2).reshape(rows, model)
    up_rows = dot(whole, w_up) * inverse2
    act = jnp.square(jax.nn.relu(up_rows)).astype(BF)
    down = dot(act, w_down).astype(BF).reshape(rows, n_all, width).transpose(1, 0, 2)
    got3 = lax.all_to_all(down, axes, 0, 0, tiled=False)
    output = (resid_float + jnp.sum(got3.astype(F32), axis=0)).astype(BF)
    return (output, new_state)


LANES = 128
SHIFT = 64
ORDERS = {
    8: (5, 7, 6, 4, 3, 1, 2, 0),
    16: (11, 12, 13, 5, 8, 0, 9, 15, 3, 2, 1, 7, 4, 14, 10, 6),
}


FIRST = {8: (5, 7, 6, 4, 3, 1, 2, 0)}


def ring(count, first=False):
    return (FIRST if first else ORDERS).get(count, tuple(range(count)))


def exchange(blocks, axes, first=False):
    group = list(ring(blocks.shape[0], first))
    return lax.all_to_all(blocks, axes, 0, 0, tiled=False, axis_index_groups=[group])


def place_kernel(out_ref):
    lane = lax.broadcasted_iota(jnp.int32, out_ref.shape, 0)
    head = lax.broadcasted_iota(jnp.int32, out_ref.shape, 1)
    out_ref[...] = jnp.where(lane == head, 1.0, 0.0).astype(BF)


def packet_line(s, j, seq, heads):
    if j < 2 * heads:
        return 2 * heads * s + j
    if j < 3 * heads:
        return 2 * heads * seq + heads * s + j - 2 * heads
    return 3 * heads * seq + s


def project_kernel(
    place_ref,
    own_ref,
    own_gain_ref,
    other_ref,
    other_gain_ref,
    wq_ref,
    wk_ref,
    wv_ref,
    wb_ref,
    wd_ref,
    out_ref,
    tokens_ref,
    pack_ref,
    *,
    n_kv,
    seq,
    heads,
):
    rows = own_ref.shape[0]
    first = lax.axis_index("tp") == 0
    own_rows = own_ref[...].astype(F32)
    other_rows = other_ref[...].astype(F32)
    tokens_ref[:rows, :] = jnp.where(first, own_rows, other_rows)
    tokens_ref[rows:, :] = jnp.where(first, other_rows, own_rows)
    own_gain = own_gain_ref[...].astype(F32)
    other_gain = other_gain_ref[...].astype(F32)
    gains = jnp.where(first, own_gain, other_gain), jnp.where(first, other_gain, own_gain)
    halves, squares = [], 0.0
    for t, gain in enumerate(gains):
        half = [tokens_ref[pl.ds(t * rows + s, n_kv, seq), :] for s in range(seq)]
        half = jnp.concatenate(half, axis=0)
        squares = squares + half * half
        halves.append((half * gain).astype(BF))
    squares = jnp.sum(squares, axis=1, keepdims=True)
    scaled = jnp.concatenate(halves, axis=1)
    dot = functools.partial(jnp.dot, preferred_element_type=F32)
    gate_weights = dot(place_ref[:, :heads], wb_ref[...])
    gate_weights = (gate_weights + dot(place_ref[:, heads:], wd_ref[...])).astype(BF)
    gates = lax.dot_general(
        scaled, gate_weights, (((1,), (1,)), ((), ())), preferred_element_type=F32
    )
    lanes = lax.broadcasted_iota(jnp.int32, (rows, LANES), 1)
    small = gates + jnp.where(lanes == 2 * heads, squares, 0.0)
    high = small.astype(BF).astype(F32)
    packet = out_ref.shape[0] // n_kv

    def pack(j, block):
        for s in range(seq):
            line = packet_line(s, j, seq, heads)
            pack_ref[pl.ds(line, n_kv, packet), :] = block[s * n_kv : (s + 1) * n_kv]

    for p, weight_ref in enumerate((wq_ref, wk_ref, wv_ref)):
        product = dot(scaled, weight_ref[...])
        for h in range(heads):
            pack(p * heads + h, product[:, h * LANES : (h + 1) * LANES])
    pack(3 * heads, high + pltpu.roll(small - high, SHIFT, 1))
    for j in range(seq * (3 * heads + 1), packet):
        pack_ref[pl.ds(j, n_kv, packet), :] = jnp.zeros((n_kv, LANES), F32)
    for k, d in enumerate(ring(n_kv, True)):
        out_ref[k * packet : (k + 1) * packet] = pack_ref[d * packet : (d + 1) * packet].astype(BF)


def delta_kernel(
    got_ref,
    state_ref,
    decay_log_ref,
    head_gain_ref,
    ff_gain_ref,
    spread_ref,
    new_ref,
    *,
    n_kv,
    seq,
    heads,
    model,
):
    packet = got_ref.shape[0] // n_kv
    total = got_ref[:packet].astype(F32)
    for d in range(1, n_kv):
        total = total + got_ref[d * packet : (d + 1) * packet].astype(F32)
    pair = 2 * heads
    stack = total[: pair * seq]
    columns = stack.T
    lengths = jnp.sum(stack * stack, axis=1, keepdims=True)
    first = 3 * heads * seq
    start = first - first % 8
    small = total[start:]
    small = small + pltpu.roll(small, LANES - SHIFT, 1)
    inverses = lax.rsqrt(small[:, pair : pair + 1] / model + 1e-06)
    lane = lax.broadcasted_iota(jnp.int32, (1, LANES), 1)
    rate = jnp.zeros((1, LANES), F32)
    for h in range(heads):
        rate = jnp.where(lane == heads + h, decay_log_ref[:, h : h + 1], rate)
    gates = inverses * small
    betas = jax.nn.sigmoid(gates)
    soft = jnp.maximum(gates, 0.0) + jnp.log1p(jnp.exp(-jnp.abs(gates)))
    keeps = jnp.exp(-jnp.exp(rate) * soft)
    row = lax.broadcasted_iota(jnp.int32, (pair, LANES), 0)
    at_lane = lax.broadcasted_iota(jnp.int32, (pair, LANES), 1)
    head = jnp.where(row < heads, row, row - heads)
    reads = []
    for s in range(seq):
        line = first - start + s
        inverse = inverses[line : line + 1]
        beta = jnp.where(at_lane == head, betas[line : line + 1], 0.0)
        beta = jnp.sum(beta, axis=1, keepdims=True)
        keep = jnp.where(at_lane == head + heads, keeps[line : line + 1], 0.0)
        keep = jnp.sum(keep, axis=1, keepdims=True)
        vectors = stack[pair * s : pair * (s + 1)]
        length = lengths[pair * s : pair * (s + 1)]
        scale = inverse * lax.rsqrt(inverse * inverse * length + 1e-06)
        high = vectors.astype(BF)
        low = (vectors - high.astype(F32)).astype(BF)
        parts = jnp.concatenate([high, low], axis=0)
        found = jnp.zeros((pair, LANES), F32)
        for h in range(heads):
            block = state_ref[s, h]
            near = block.astype(BF)
            rest = (block - near.astype(F32)).astype(BF)
            both = jnp.dot(parts, near, preferred_element_type=F32)
            both = both + jnp.dot(parts, rest, preferred_element_type=F32)
            found = jnp.where(head == h, both[:pair] + both[pair:], found)
        found = found * (keep * scale)
        value = inverse * total[pair * seq + heads * s : pair * seq + heads * (s + 1)]
        change = (beta[:heads] * scale[heads:]) * (value - found[heads:])
        cross = jnp.sum(vectors[:heads] * vectors[heads:], axis=1, keepdims=True)
        reads.append(found[:heads] + (scale[:heads] * cross) * change)
        for h in range(heads):
            kcol = columns[:, pair * s + heads + h : pair * s + heads + h + 1]
            new_ref[s, h] = keep[h : h + 1] * state_ref[s, h] + kcol * change[h : h + 1]
    read = jnp.concatenate(reads, axis=0) / jnp.sqrt(jnp.float32(LANES))
    normed = (
        read
        * lax.rsqrt(jnp.mean(read * read, axis=1, keepdims=True) + 1e-06)
        * head_gain_ref[...].astype(F32)
    )
    lines = spread_ref.shape[1]
    fill = lines - seq * heads
    sent = jnp.concatenate(
        [normed, jnp.broadcast_to(ff_gain_ref[...].astype(F32), (fill, LANES))], axis=0
    ).astype(BF)
    for d in range(spread_ref.shape[0]):
        spread_ref[d] = sent


def mix_kernel(
    got_ref,
    tokens_ref,
    other_tokens_ref,
    own_ref,
    other_ref,
    spread_ref,
    resid_ref,
    rows_ref,
    mixed_ref,
    *,
    n_kv,
    n_tp,
    seq,
    heads,
):
    lines = got_ref.shape[0] // (n_kv * n_tp)
    rows, width = tokens_ref.shape
    for k, member in enumerate(ring(n_kv * n_tp)):
        at = ((member % n_tp) * n_kv + member // n_tp) * lines
        rows_ref[at : at + lines] = got_ref[k * lines : (k + 1) * lines].astype(F32)
    dot = functools.partial(jnp.dot, preferred_element_type=F32)
    halves = []
    for t in range(n_tp):
        blocks = []
        for h in range(heads):
            parts = [
                rows_ref[pl.ds(t * n_kv * lines + s * heads + h, n_kv, lines), :] for s in range(seq)
            ]
            blocks.append(jnp.concatenate(parts, axis=0))
        halves.append(jnp.concatenate(blocks, axis=1))
    first = lax.axis_index("tp") == 0
    own = jnp.where(first, halves[0], halves[1]).astype(BF)
    other = jnp.where(first, halves[1], halves[0]).astype(BF)
    mixed = dot(own, own_ref[...]).astype(BF).astype(F32)
    mixed = mixed + dot(other, other_ref[...]).astype(BF).astype(F32)
    own_tokens = tokens_ref[...].astype(F32)
    other_tokens = other_tokens_ref[...].astype(F32)
    tokens = jnp.where(first, own_tokens, other_tokens), jnp.where(first, other_tokens, own_tokens)
    resids = []
    for t in range(n_tp):
        for s in range(seq):
            mixed_ref[pl.ds(t * rows + s, n_kv, seq), :] = mixed[
                s * n_kv : (s + 1) * n_kv, t * width : (t + 1) * width
            ]
        resids.append(tokens[t] + mixed_ref[t * rows : (t + 1) * rows, :])
    resid_ref[...] = jnp.where(first, resids[0], resids[1]).astype(BF)
    resid = jnp.concatenate(resids, axis=1).astype(BF)
    for d in range(n_kv):
        spread_ref[d] = resid


def feed_kernel(
    got_ref,
    gains_ref,
    up_ref,
    down_ref,
    state_ref,
    out_ref,
    new_ref,
    sems,
    *,
    gain_line,
    model,
    n_tp,
):
    copies = [
        pltpu.make_async_copy(state_ref.at[n, m], new_ref.at[n, m], sems.at[n, m])
        for n in range(state_ref.shape[0])
        for m in range(state_ref.shape[1])
    ]
    for copy in copies:
        copy.start()
    n_all, rows, width = out_ref.shape
    n_kv = n_all // n_tp
    lines = gains_ref.shape[0] // n_all
    squares = jnp.zeros((rows, n_tp * width), F32)
    blocks = []
    for d in range(n_kv):
        block = got_ref[ring(n_kv).index(d)].astype(F32)
        squares = squares + block * block
        starts = [ring(n_all).index(d * n_tp + t) * lines for t in range(n_tp)]
        gain = [
            gains_ref[at : at + lines].astype(F32)[gain_line : gain_line + 1] for at in starts
        ]
        blocks.append((block * jnp.concatenate(gain, axis=1)).astype(BF))
    inverse = lax.rsqrt(jnp.sum(squares, axis=1, keepdims=True) / model + 1e-06)
    scaled = jnp.concatenate(blocks, axis=1)
    up = jnp.dot(scaled, up_ref[...], preferred_element_type=F32) * inverse
    up = jnp.maximum(up, 0.0)
    act = (up * up).astype(BF)
    down = jnp.dot(act, down_ref[...], preferred_element_type=F32)
    for k, at in enumerate(ring(n_all)):
        out_ref[k] = down[:, at * width : (at + 1) * width].astype(BF)
    for copy in copies:
        copy.wait()


def fused(
    tokens,
    state,
    mix_gain,
    w_query,
    w_key,
    w_value,
    w_beta,
    w_decay,
    decay_log,
    head_gain,
    w_out,
    ff_gain,
    w_up,
    w_down,
    n_kv,
    n_tp,
):
    rows, width = tokens.shape
    seq, heads, size = state.shape[:3]
    n_all = n_kv * n_tp
    model = width * n_all
    keys = heads * size
    per_seq = 3 * heads + 1
    packet = -(-seq * per_seq // 8) * 8
    lines = -(-(seq * heads + 1) // 8) * 8
    axes = ("kv", "tp")
    swap = [(i, n_tp - 1 - i) for i in range(n_tp)]
    shape = jax.ShapeDtypeStruct
    vmem = pl.BlockSpec(memory_space=pltpu.VMEM)
    cost = pl.CostEstimate(flops=4 * 10**9, bytes_accessed=8 * 10**6, transcendentals=0)
    params = pltpu.CompilerParams(vmem_limit_bytes=16 * 1024 * 1024)

    gain_row = mix_gain[None, :]
    other_tokens = lax.ppermute(tokens, "tp", swap)
    other_gain = lax.ppermute(gain_row, "tp", swap)
    hbm = pl.BlockSpec(memory_space=pltpu.HBM)
    other_out = lax.ppermute(w_out, "tp", swap)
    place = pl.pallas_call(
        place_kernel,
        out_shape=shape((LANES, 2 * heads), BF),
        out_specs=vmem,
        name="place",
        cost_estimate=cost,
        compiler_params=params,
    )()

    sent = pl.pallas_call(
        functools.partial(project_kernel, n_kv=n_kv, seq=seq, heads=heads),
        out_shape=shape((n_kv * packet, LANES), BF),
        in_specs=[vmem] * 10,
        out_specs=vmem,
        scratch_shapes=[
            pltpu.VMEM((n_tp * rows, LANES), F32),
            pltpu.VMEM((n_kv * packet, LANES), F32),
        ],
        name="project",
        cost_estimate=cost,
        compiler_params=params,
    )(
        place,
        tokens,
        gain_row,
        other_tokens,
        other_gain,
        w_query,
        w_key,
        w_value,
        w_beta.T,
        w_decay.T,
    )
    sent, other_out = lax.optimization_barrier((sent, other_out))
    got = exchange(sent.reshape(n_kv, packet, LANES), "kv", True)
    spread, new_state = pl.pallas_call(
        functools.partial(delta_kernel, n_kv=n_kv, seq=seq, heads=heads, model=model),
        out_shape=(shape((n_all, lines, LANES), BF), shape(state.shape, F32)),
        in_specs=[vmem] * 5,
        out_specs=(vmem, vmem),
        name="delta",
        cost_estimate=cost,
        compiler_params=params,
    )(got.reshape(n_kv * packet, LANES), state, decay_log[None, :], head_gain[None, :], ff_gain[None, :])
    got = exchange(spread, axes).reshape(n_all * lines, LANES)
    spread, resid = pl.pallas_call(
        functools.partial(mix_kernel, n_kv=n_kv, n_tp=n_tp, seq=seq, heads=heads),
        out_shape=(shape((n_kv, rows, n_tp * width), BF), shape((rows, width), BF)),
        in_specs=[vmem] * 5,
        out_specs=(vmem, vmem),
        scratch_shapes=[
            pltpu.VMEM((n_all * lines, LANES), F32),
            pltpu.VMEM((n_tp * rows, width), F32),
        ],
        name="mix",
        cost_estimate=cost,
        compiler_params=params,
    )(got, tokens, other_tokens, w_out, other_out)
    got2 = exchange(spread, "kv")
    down, new_state = pl.pallas_call(
        functools.partial(feed_kernel, gain_line=seq * heads, model=model, n_tp=n_tp),
        out_shape=(shape((n_all, rows, width), BF), shape(state.shape, F32)),
        in_specs=[vmem] * 5,
        out_specs=(vmem, hbm),
        scratch_shapes=[pltpu.SemaphoreType.DMA((seq, heads))],
        name="feed",
        compiler_params=params,
    )(got2, got, w_up, w_down, new_state)
    got3 = exchange(down, axes)
    output = (resid.astype(F32) + jnp.sum(got3.astype(F32), axis=0)).astype(BF)
    return (output, new_state)


def local(*arrays, n_kv, n_tp):
    tokens, state = arrays[:2]
    whole_tiles = tokens.shape[1] == LANES and state.shape[2] == LANES and n_kv % 8 == 0 and n_tp == 2
    form = fused if whole_tiles else plain
    return form(*arrays, n_kv=n_kv, n_tp=n_tp)


def solution(mesh):
    placed = (
        P("dp", ("kv", "tp")),
        P(("dp", "kv"), "tp", None, None),
        P(("kv", "tp")),
        P("kv", "tp"),
        P("kv", "tp"),
        P("kv", "tp"),
        P("kv", "tp"),
        P("kv", "tp"),
        P("tp"),
        P(),
        P("tp", "kv"),
        P(("kv", "tp")),
        P(None, ("kv", "tp")),
        P(("kv", "tp"), None),
    )
    return jax.shard_map(
        functools.partial(local, n_kv=mesh.shape["kv"], n_tp=mesh.shape["tp"]),
        mesh=mesh,
        in_specs=placed,
        out_specs=(P("dp", ("kv", "tp")), P(("dp", "kv"), "tp", None, None)),
        check_vma=False,
    )
```

```python
import functools

import jax
import jax.numpy as jnp
from jax import lax
from jax.experimental import pallas as pl
from jax.experimental.pallas import tpu as pltpu
from jax.sharding import PartitionSpec as P

BF = jnp.bfloat16
F32 = jnp.float32


def split_pair(value):
    high = value.astype(BF)
    low = (value - lax.reduce_precision(value, 8, 7)).astype(BF)
    return high, low


def plain(
    tokens,
    state,
    mix_gain,
    w_query,
    w_key,
    w_value,
    w_beta,
    w_decay,
    decay_log,
    head_gain,
    w_out,
    ff_gain,
    w_up,
    w_down,
    n_kv,
    n_tp,
):
    rows, width = tokens.shape
    seq, heads, size = state.shape[:3]
    n_all = n_kv * n_tp
    model = width * n_all
    keys = heads * size

    packed = jnp.concatenate([tokens, mix_gain[None, :]], axis=0)
    wide = lax.all_gather(packed, "tp", axis=1, tiled=True)
    tp_at = lax.axis_index("tp")
    out_cols = []
    for step in range(n_tp):
        target = (tp_at + step) % n_tp
        block = lax.dynamic_slice_in_dim(w_out, target * width, width, axis=1)
        if step:
            block = lax.ppermute(block, "tp", [(i, (i + step) % n_tp) for i in range(n_tp)])
        out_cols.append(block)

    wide_float = wide[:rows].astype(F32)
    scaled = (wide_float * wide[rows:].astype(F32)).astype(BF)
    dot = functools.partial(jnp.dot, preferred_element_type=F32)
    gates_part = dot(scaled, jnp.concatenate([w_beta, w_decay], axis=1))
    square_part = jnp.sum(wide_float * wide_float, axis=1, keepdims=True)
    small = jnp.concatenate([gates_part, square_part], axis=1)
    high, low = split_pair(small)
    n_small = small.shape[1]
    pad = jnp.zeros((rows, size - 2 * n_small), BF)
    sent = jnp.concatenate(
        [
            dot(scaled, w_query).astype(BF),
            dot(scaled, w_key).astype(BF),
            dot(scaled, w_value).astype(BF),
            high,
            low,
            pad,
        ],
        axis=1,
    ).reshape(n_kv, seq, 3 * keys + size)
    got = lax.all_to_all(sent, "kv", 0, 0, tiled=False)
    total = jnp.sum(got.astype(F32), axis=0)
    small = total[:, 3 * keys : 3 * keys + n_small] + total[:, 3 * keys + n_small : 3 * keys + 2 * n_small]
    inverse = lax.rsqrt(small[:, 2 * heads :] / model + 1e-06)
    query = (inverse * total[:, :keys]).reshape(seq, heads, size)
    key_rows = (inverse * total[:, keys : 2 * keys]).reshape(seq, heads, size)
    value = (inverse * total[:, 2 * keys : 3 * keys]).reshape(seq, heads, size)
    beta = jax.nn.sigmoid(inverse * small[:, :heads])
    decay = -jnp.exp(decay_log)[None, :] * jax.nn.softplus(inverse * small[:, heads : 2 * heads])
    qnorm = query * lax.rsqrt(jnp.sum(query * query, axis=-1, keepdims=True) + 1e-06)
    knorm = key_rows * lax.rsqrt(jnp.sum(key_rows * key_rows, axis=-1, keepdims=True) + 1e-06)
    kept = state * jnp.exp(decay)[:, :, None, None]
    predicted = jnp.sum(kept * knorm[:, :, :, None], axis=2)
    new_state = kept + (beta[:, :, None] * knorm)[:, :, :, None] * (value - predicted)[:, :, None, :]
    read = jnp.sum(new_state * qnorm[:, :, :, None], axis=2) / jnp.sqrt(jnp.float32(size))
    normed = (
        read
        * lax.rsqrt(jnp.mean(read * read, axis=-1, keepdims=True) + 1e-06)
        * head_gain.astype(F32)
    )
    normed = normed.astype(BF).reshape(seq, keys)
    axes = ("kv", "tp")
    spread = lax.all_to_all(jnp.broadcast_to(normed[None], (n_all, seq, keys)), axes, 0, 0, tiled=False)
    spread = spread.reshape(n_kv, n_tp, seq, keys)
    mixed = 0.0
    for step in range(n_tp):
        heads_of = lax.dynamic_index_in_dim(spread, (tp_at - step) % n_tp, 1, keepdims=False)
        part = dot(heads_of.reshape(rows, keys), out_cols[step])
        mixed = mixed + lax.reduce_precision(part, 8, 7)
    resid = (tokens.astype(F32) + mixed).astype(BF)
    resid_float = resid.astype(F32)
    scaled2 = (resid_float * ff_gain.astype(F32)[None, :]).astype(BF)
    high, low = split_pair(jnp.sum(resid_float * resid_float, axis=1))
    tail_rows = -(-2 * rows // width // 8) * 8
    tail = jnp.concatenate([high, low, jnp.zeros((tail_rows * width - 2 * rows,), BF)])
    tail = tail.reshape(tail_rows, width)
    sent2 = jnp.concatenate([scaled2, tail], axis=0)
    got2 = lax.all_to_all(jnp.broadcast_to(sent2[None], (n_all,) + sent2.shape), axes, 0, 0, tiled=False)
    sums = jnp.sum(got2[:, rows:].reshape(n_all, tail_rows * width)[:, : 2 * rows].astype(F32), axis=0)
    inverse2 = lax.rsqrt((sums[:rows] + sums[rows:]) / model + 1e-06)[:, None]
    whole = got2[:, :rows].transpose(1, 0, 2).reshape(rows, model)
    up_rows = dot(whole, w_up) * inverse2
    act = jnp.square(jax.nn.relu(up_rows)).astype(BF)
    down = dot(act, w_down).astype(BF).reshape(rows, n_all, width).transpose(1, 0, 2)
    got3 = lax.all_to_all(down, axes, 0, 0, tiled=False)
    output = (resid_float + jnp.sum(got3.astype(F32), axis=0)).astype(BF)
    return (output, new_state)


LANES = 128
SHIFT = 64
ORDERS = {
    8: (5, 7, 6, 4, 3, 1, 2, 0),
    16: (11, 12, 13, 5, 8, 0, 9, 15, 3, 2, 1, 7, 4, 14, 10, 6),
}


FIRST = {8: (5, 7, 6, 4, 3, 1, 2, 0)}


def ring(count, first=False):
    return (FIRST if first else ORDERS).get(count, tuple(range(count)))


def exchange(blocks, axes, first=False):
    group = list(ring(blocks.shape[0], first))
    return lax.all_to_all(blocks, axes, 0, 0, tiled=False, axis_index_groups=[group])


def place_kernel(out_ref):
    lane = lax.broadcasted_iota(jnp.int32, out_ref.shape, 0)
    head = lax.broadcasted_iota(jnp.int32, out_ref.shape, 1)
    out_ref[...] = jnp.where(lane == head, 1.0, 0.0).astype(BF)


def packet_line(s, j, seq, heads):
    if j < 2 * heads:
        return 2 * heads * s + j
    if j < 3 * heads:
        return 2 * heads * seq + heads * s + j - 2 * heads
    return 3 * heads * seq + s


def project_kernel(
    place_ref,
    own_ref,
    own_gain_ref,
    other_ref,
    other_gain_ref,
    wq_ref,
    wk_ref,
    wv_ref,
    wb_ref,
    wd_ref,
    out_ref,
    tokens_ref,
    pack_ref,
    *,
    n_kv,
    seq,
    heads,
):
    rows = own_ref.shape[0]
    first = lax.axis_index("tp") == 0
    own_rows = own_ref[...].astype(F32)
    other_rows = other_ref[...].astype(F32)
    tokens_ref[:rows, :] = jnp.where(first, own_rows, other_rows)
    tokens_ref[rows:, :] = jnp.where(first, other_rows, own_rows)
    own_gain = own_gain_ref[...].astype(F32)
    other_gain = other_gain_ref[...].astype(F32)
    gains = jnp.where(first, own_gain, other_gain), jnp.where(first, other_gain, own_gain)
    halves, squares = [], 0.0
    for t, gain in enumerate(gains):
        half = [tokens_ref[pl.ds(t * rows + s, n_kv, seq), :] for s in range(seq)]
        half = jnp.concatenate(half, axis=0)
        squares = squares + half * half
        halves.append((half * gain).astype(BF))
    squares = jnp.sum(squares, axis=1, keepdims=True)
    scaled = jnp.concatenate(halves, axis=1)
    dot = functools.partial(jnp.dot, preferred_element_type=F32)
    gate_weights = dot(place_ref[:, :heads], wb_ref[...])
    gate_weights = (gate_weights + dot(place_ref[:, heads:], wd_ref[...])).astype(BF)
    gates = lax.dot_general(
        scaled, gate_weights, (((1,), (1,)), ((), ())), preferred_element_type=F32
    )
    lanes = lax.broadcasted_iota(jnp.int32, (rows, LANES), 1)
    small = gates + jnp.where(lanes == 2 * heads, squares, 0.0)
    high = small.astype(BF).astype(F32)
    packet = out_ref.shape[0] // n_kv

    def pack(j, block):
        for s in range(seq):
            line = packet_line(s, j, seq, heads)
            pack_ref[pl.ds(line, n_kv, packet), :] = block[s * n_kv : (s + 1) * n_kv]

    for p, weight_ref in enumerate((wq_ref, wk_ref, wv_ref)):
        product = dot(scaled, weight_ref[...])
        for h in range(heads):
            pack(p * heads + h, product[:, h * LANES : (h + 1) * LANES])
    pack(3 * heads, high + pltpu.roll(small - high, SHIFT, 1))
    for j in range(seq * (3 * heads + 1), packet):
        pack_ref[pl.ds(j, n_kv, packet), :] = jnp.zeros((n_kv, LANES), F32)
    for k, d in enumerate(ring(n_kv, True)):
        out_ref[k * packet : (k + 1) * packet] = pack_ref[d * packet : (d + 1) * packet].astype(BF)


def delta_kernel(
    got_ref,
    state_ref,
    decay_log_ref,
    head_gain_ref,
    ff_gain_ref,
    spread_ref,
    new_ref,
    *,
    n_kv,
    seq,
    heads,
    model,
):
    packet = got_ref.shape[0] // n_kv
    total = got_ref[:packet].astype(F32)
    for d in range(1, n_kv):
        total = total + got_ref[d * packet : (d + 1) * packet].astype(F32)
    pair = 2 * heads
    stack = total[: pair * seq]
    columns = stack.T
    lengths = jnp.sum(stack * stack, axis=1, keepdims=True)
    first = 3 * heads * seq
    start = first - first % 8
    small = total[start:]
    small = small + pltpu.roll(small, LANES - SHIFT, 1)
    inverses = lax.rsqrt(small[:, pair : pair + 1] / model + 1e-06)
    lane = lax.broadcasted_iota(jnp.int32, (1, LANES), 1)
    rate = jnp.zeros((1, LANES), F32)
    for h in range(heads):
        rate = jnp.where(lane == heads + h, decay_log_ref[:, h : h + 1], rate)
    gates = inverses * small
    betas = jax.nn.sigmoid(gates)
    soft = jnp.maximum(gates, 0.0) + jnp.log1p(jnp.exp(-jnp.abs(gates)))
    keeps = jnp.exp(-jnp.exp(rate) * soft)
    row = lax.broadcasted_iota(jnp.int32, (pair, LANES), 0)
    at_lane = lax.broadcasted_iota(jnp.int32, (pair, LANES), 1)
    head = jnp.where(row < heads, row, row - heads)
    reads = []
    for s in range(seq):
        line = first - start + s
        inverse = inverses[line : line + 1]
        beta = jnp.where(at_lane == head, betas[line : line + 1], 0.0)
        beta = jnp.sum(beta, axis=1, keepdims=True)
        keep = jnp.where(at_lane == head + heads, keeps[line : line + 1], 0.0)
        keep = jnp.sum(keep, axis=1, keepdims=True)
        vectors = stack[pair * s : pair * (s + 1)]
        length = lengths[pair * s : pair * (s + 1)]
        scale = inverse * lax.rsqrt(inverse * inverse * length + 1e-06)
        high = vectors.astype(BF)
        low = (vectors - high.astype(F32)).astype(BF)
        parts = jnp.concatenate([high, low], axis=0)
        found = jnp.zeros((pair, LANES), F32)
        for h in range(heads):
            block = state_ref[s, h]
            near = block.astype(BF)
            rest = (block - near.astype(F32)).astype(BF)
            both = jnp.dot(parts, near, preferred_element_type=F32)
            both = both + jnp.dot(parts, rest, preferred_element_type=F32)
            found = jnp.where(head == h, both[:pair] + both[pair:], found)
        found = found * (keep * scale)
        value = inverse * total[pair * seq + heads * s : pair * seq + heads * (s + 1)]
        change = (beta[:heads] * scale[heads:]) * (value - found[heads:])
        cross = jnp.sum(vectors[:heads] * vectors[heads:], axis=1, keepdims=True)
        reads.append(found[:heads] + (scale[:heads] * cross) * change)
        for h in range(heads):
            kcol = columns[:, pair * s + heads + h : pair * s + heads + h + 1]
            new_ref[s, h] = keep[h : h + 1] * state_ref[s, h] + kcol * change[h : h + 1]
    read = jnp.concatenate(reads, axis=0) / jnp.sqrt(jnp.float32(LANES))
    normed = (
        read
        * lax.rsqrt(jnp.mean(read * read, axis=1, keepdims=True) + 1e-06)
        * head_gain_ref[...].astype(F32)
    )
    lines = spread_ref.shape[1]
    fill = lines - seq * heads
    sent = jnp.concatenate(
        [normed, jnp.broadcast_to(ff_gain_ref[...].astype(F32), (fill, LANES))], axis=0
    ).astype(BF)
    for d in range(spread_ref.shape[0]):
        spread_ref[d] = sent


def mix_kernel(
    got_ref,
    tokens_ref,
    other_tokens_ref,
    own_ref,
    other_ref,
    spread_ref,
    resid_ref,
    rows_ref,
    mixed_ref,
    *,
    n_kv,
    n_tp,
    seq,
    heads,
):
    lines = got_ref.shape[0] // (n_kv * n_tp)
    rows, width = tokens_ref.shape
    for k, member in enumerate(ring(n_kv * n_tp)):
        at = ((member % n_tp) * n_kv + member // n_tp) * lines
        rows_ref[at : at + lines] = got_ref[k * lines : (k + 1) * lines].astype(F32)
    dot = functools.partial(jnp.dot, preferred_element_type=F32)
    halves = []
    for t in range(n_tp):
        blocks = []
        for h in range(heads):
            parts = [
                rows_ref[pl.ds(t * n_kv * lines + s * heads + h, n_kv, lines), :] for s in range(seq)
            ]
            blocks.append(jnp.concatenate(parts, axis=0))
        halves.append(jnp.concatenate(blocks, axis=1))
    first = lax.axis_index("tp") == 0
    own = jnp.where(first, halves[0], halves[1]).astype(BF)
    other = jnp.where(first, halves[1], halves[0]).astype(BF)
    mixed = dot(own, own_ref[...]).astype(BF).astype(F32)
    mixed = mixed + dot(other, other_ref[...]).astype(BF).astype(F32)
    own_tokens = tokens_ref[...].astype(F32)
    other_tokens = other_tokens_ref[...].astype(F32)
    tokens = jnp.where(first, own_tokens, other_tokens), jnp.where(first, other_tokens, own_tokens)
    resids = []
    for t in range(n_tp):
        for s in range(seq):
            mixed_ref[pl.ds(t * rows + s, n_kv, seq), :] = mixed[
                s * n_kv : (s + 1) * n_kv, t * width : (t + 1) * width
            ]
        resids.append(tokens[t] + mixed_ref[t * rows : (t + 1) * rows, :])
    resid_ref[...] = jnp.where(first, resids[0], resids[1]).astype(BF)
    resid = jnp.concatenate(resids, axis=1).astype(BF)
    for d in range(n_kv):
        spread_ref[d] = resid


def feed_kernel(
    got_ref,
    gains_ref,
    up_ref,
    down_ref,
    state_ref,
    out_ref,
    new_ref,
    sems,
    *,
    gain_line,
    model,
    n_tp,
):
    copies = [
        pltpu.make_async_copy(state_ref.at[n, m], new_ref.at[n, m], sems.at[n, m])
        for n in range(state_ref.shape[0])
        for m in range(state_ref.shape[1])
    ]
    for copy in copies:
        copy.start()
    n_all, rows, width = out_ref.shape
    n_kv = n_all // n_tp
    lines = gains_ref.shape[0] // n_all
    squares = jnp.zeros((rows, n_tp * width), F32)
    blocks = []
    for d in range(n_kv):
        block = got_ref[ring(n_kv).index(d)].astype(F32)
        squares = squares + block * block
        starts = [ring(n_all).index(d * n_tp + t) * lines for t in range(n_tp)]
        gain = [
            gains_ref[at : at + lines].astype(F32)[gain_line : gain_line + 1] for at in starts
        ]
        blocks.append((block * jnp.concatenate(gain, axis=1)).astype(BF))
    inverse = lax.rsqrt(jnp.sum(squares, axis=1, keepdims=True) / model + 1e-06)
    scaled = jnp.concatenate(blocks, axis=1)
    up = jnp.dot(scaled, up_ref[...], preferred_element_type=F32) * inverse
    up = jnp.maximum(up, 0.0)
    act = (up * up).astype(BF)
    down = jnp.dot(act, down_ref[...], preferred_element_type=F32)
    for k, at in enumerate(ring(n_all)):
        out_ref[k] = down[:, at * width : (at + 1) * width].astype(BF)
    for copy in copies:
        copy.wait()


def fused(
    tokens,
    state,
    mix_gain,
    w_query,
    w_key,
    w_value,
    w_beta,
    w_decay,
    decay_log,
    head_gain,
    w_out,
    ff_gain,
    w_up,
    w_down,
    n_kv,
    n_tp,
):
    rows, width = tokens.shape
    seq, heads, size = state.shape[:3]
    n_all = n_kv * n_tp
    model = width * n_all
    keys = heads * size
    per_seq = 3 * heads + 1
    packet = -(-seq * per_seq // 8) * 8
    lines = -(-(seq * heads + 1) // 8) * 8
    axes = ("kv", "tp")
    swap = [(i, n_tp - 1 - i) for i in range(n_tp)]
    shape = jax.ShapeDtypeStruct
    vmem = pl.BlockSpec(memory_space=pltpu.VMEM)
    cost = pl.CostEstimate(flops=4 * 10**9, bytes_accessed=8 * 10**6, transcendentals=0)
    params = pltpu.CompilerParams(vmem_limit_bytes=16 * 1024 * 1024)

    gain_row = mix_gain[None, :]
    other_tokens = lax.ppermute(tokens, "tp", swap)
    other_gain = lax.ppermute(gain_row, "tp", swap)
    hbm = pl.BlockSpec(memory_space=pltpu.HBM)
    other_out = lax.ppermute(w_out, "tp", swap)
    place = pl.pallas_call(
        place_kernel,
        out_shape=shape((LANES, 2 * heads), BF),
        out_specs=vmem,
        name="place",
        cost_estimate=cost,
        compiler_params=params,
    )()

    sent = pl.pallas_call(
        functools.partial(project_kernel, n_kv=n_kv, seq=seq, heads=heads),
        out_shape=shape((n_kv * packet, LANES), BF),
        in_specs=[vmem] * 10,
        out_specs=vmem,
        scratch_shapes=[
            pltpu.VMEM((n_tp * rows, LANES), F32),
            pltpu.VMEM((n_kv * packet, LANES), F32),
        ],
        name="project",
        cost_estimate=cost,
        compiler_params=params,
    )(
        place,
        tokens,
        gain_row,
        other_tokens,
        other_gain,
        w_query,
        w_key,
        w_value,
        w_beta.T,
        w_decay.T,
    )
    got = exchange(sent.reshape(n_kv, packet, LANES), "kv", True)
    got, other_out = lax.optimization_barrier((got, other_out))
    spread, new_state = pl.pallas_call(
        functools.partial(delta_kernel, n_kv=n_kv, seq=seq, heads=heads, model=model),
        out_shape=(shape((n_all, lines, LANES), BF), shape(state.shape, F32)),
        in_specs=[vmem] * 5,
        out_specs=(vmem, vmem),
        name="delta",
        cost_estimate=cost,
        compiler_params=params,
    )(got.reshape(n_kv * packet, LANES), state, decay_log[None, :], head_gain[None, :], ff_gain[None, :])
    got = exchange(spread, axes).reshape(n_all * lines, LANES)
    spread, resid = pl.pallas_call(
        functools.partial(mix_kernel, n_kv=n_kv, n_tp=n_tp, seq=seq, heads=heads),
        out_shape=(shape((n_kv, rows, n_tp * width), BF), shape((rows, width), BF)),
        in_specs=[vmem] * 5,
        out_specs=(vmem, vmem),
        scratch_shapes=[
            pltpu.VMEM((n_all * lines, LANES), F32),
            pltpu.VMEM((n_tp * rows, width), F32),
        ],
        name="mix",
        cost_estimate=cost,
        compiler_params=params,
    )(got, tokens, other_tokens, w_out, other_out)
    got2 = exchange(spread, "kv")
    down, new_state = pl.pallas_call(
        functools.partial(feed_kernel, gain_line=seq * heads, model=model, n_tp=n_tp),
        out_shape=(shape((n_all, rows, width), BF), shape(state.shape, F32)),
        in_specs=[vmem] * 5,
        out_specs=(vmem, hbm),
        scratch_shapes=[pltpu.SemaphoreType.DMA((seq, heads))],
        name="feed",
        compiler_params=params,
    )(got2, got, w_up, w_down, new_state)
    got3 = exchange(down, axes)
    output = (resid.astype(F32) + jnp.sum(got3.astype(F32), axis=0)).astype(BF)
    return (output, new_state)


def local(*arrays, n_kv, n_tp):
    tokens, state = arrays[:2]
    whole_tiles = tokens.shape[1] == LANES and state.shape[2] == LANES and n_kv % 8 == 0 and n_tp == 2
    form = fused if whole_tiles else plain
    return form(*arrays, n_kv=n_kv, n_tp=n_tp)


def solution(mesh):
    placed = (
        P("dp", ("kv", "tp")),
        P(("dp", "kv"), "tp", None, None),
        P(("kv", "tp")),
        P("kv", "tp"),
        P("kv", "tp"),
        P("kv", "tp"),
        P("kv", "tp"),
        P("kv", "tp"),
        P("tp"),
        P(),
        P("tp", "kv"),
        P(("kv", "tp")),
        P(None, ("kv", "tp")),
        P(("kv", "tp"), None),
    )
    return jax.shard_map(
        functools.partial(local, n_kv=mesh.shape["kv"], n_tp=mesh.shape["tp"]),
        mesh=mesh,
        in_specs=placed,
        out_specs=(P("dp", ("kv", "tp")), P(("dp", "kv"), "tp", None, None)),
        check_vma=False,
    )
```
